256 devices in a mesh: rep: 2 (over z_hi), fs: 16 (over z_lo, x), tp: 8 (over y, core).
Axes of the slice: x: 4, y: 4, z: 8 (z_hi: 2, z_lo: 4; z = z_hi * 4 + z_lo), core: 2. Of those that a mesh axis runs over, the one named last changes fastest.
Arguments:
- tokens: bfloat16 [32768, 2048], P(('rep', 'fs', 'tp')), may hold values from -6 to 6
- mixer_gain: float32 [2048], replicated, may hold values from 0.1 to 1.9
- direct_weight: float32 [2048, 1024], P('fs', 'tp'), may hold values from -0.125 to 0.125
- direct_scale: float32 [1024], P('tp'), may hold values from 0.5 to 2
- value_weight: float32 [2048, 1024], P('fs', 'tp'), may hold values from -0.125 to 0.125
- value_scale: float32 [1024], P('tp'), may hold values from 0.5 to 8, as said below
- value_gain: float32 [1024], P('tp'), may hold values from 0.1 to 1.9
- value_shift: float32 [1024], P('tp'), may hold values from -3 to 3
- spatial_weight: bfloat16 [16, 128, 128], P('tp'), may hold values from -0.25 to 0.25
- spatial_bias: float32 [16, 128], P('tp'), may hold values from 0.1 to 1.9
- merge_weight: float32 [1024, 2048], P('tp', 'fs'), may hold values from -0.1875 to 0.1875
- merge_scale: float32 [2048], P('fs'), may hold values from 0.5 to 2
- channel_gain: float32 [2048], replicated, may hold values from 0.1 to 1.9
- expand_weight: float32 [2048, 8192], P('fs', 'tp'), may hold values from -0.125 to 0.125
- expand_scale: float32 [8192], P('tp'), may hold values from 0.5 to 2
- reduce_weight: float32 [8192, 2048], P('tp', 'fs'), may hold values from -0.0625 to 0.0625
- reduce_scale: float32 [2048], P('fs'), may hold values from 0.5 to 2
Outputs:
- result: bfloat16 [32768, 2048], P(('rep', 'fs', 'tp'))
The draws below stay inside these ranges and needn't reach their ends.
Inputs may be any that keep to these rules, and one draw needn't show every extreme that they name: `value_scale`: positive column scales.
All inputs are finite; a program needn't handle non-finite values.
Results may differ from the reference program's by a relative error of at most 0.024.
Values may be sent and summed in bfloat16 or wider, within the bound.
No kernel may reach another device: no remote copies, remote signals or barrier semaphores. Data moves between devices by JAX's collectives and lax.ppermute only.
A program may use at most 64 MiB of HBM per device.

```python
import math
import jax
import jax.numpy as jnp
from jax import lax

D = 2048
GROUPS = 16
GDIM = 64
AW = 1024
FF = 8192
BLOCK = 128
TOK_DEV = 128
TOKENS = 32768
N_TP = 8


def draw_value_scale(key, part):
    ramp = jnp.exp(jnp.log(4.0) * jnp.arange(AW, dtype=jnp.float32) / (AW - 1))
    factor = jnp.exp(jax.random.uniform(key, (AW,), jnp.float32, jnp.log(0.7), jnp.log(1.4)))
    return ramp * factor


def levels(stream_key, shape, shards, low, top_value):
    level = 1.0
    for axis_at, blocks in shards:
        draws = jax.random.uniform(jax.random.fold_in(jax.random.fold_in(stream_key, 6), axis_at), (blocks,), jnp.float32, low / len(shards), top_value / len(shards))
        level = level * jnp.repeat(jnp.exp(draws), shape[axis_at] // blocks).reshape((-1,) + (1,) * (len(shape) - 1 - axis_at))
    return level


def scatter_about(rng, extent, deviation, bound, shards=(), kind=jnp.bfloat16):
    result = jax.random.normal(rng, extent, jnp.float32) * deviation
    if len(shards) > 0:
        result = levels(rng, extent, shards, -0.22, 0.18) * result
    return jnp.clip(result, min=-bound, max=bound).astype(kind)


def setup_inputs(seed: int = 0) -> dict:
    seeds = jax.random.split(jax.random.key(seed), 18)
    tokens = scatter_about(seeds[0], (TOKENS, D), 1.0, 6.0, ((0, 256),))
    mixer_gain = jnp.clip(1.0 + 0.18 * jax.random.normal(seeds[1], (D,), jnp.float32), 0.1, 1.9)
    direct_weight = scatter_about(seeds[2], (D, AW), D ** -0.5, 0.125, ((0, 16), (1, 8)), jnp.float32)
    direct_scale = jnp.clip(jnp.exp(math.log(2.0) - 1.3862944 * jax.random.uniform(seeds[3], (AW,), jnp.float32) ** levels(seeds[3], (AW,), ((0, 8),), -0.2, 0.2)), 0.5, 2.0)
    value_weight = scatter_about(seeds[4], (D, AW), D ** -0.5, 0.125, ((0, 16), (1, 8)), jnp.float32)
    value_scale = draw_value_scale(jax.random.fold_in(seeds[17], 71), 0)
    value_gain = jnp.clip(1.0 + 0.18 * jax.random.normal(seeds[6], (AW,), jnp.float32), 0.1, 1.9)
    value_shift = scatter_about(seeds[7], (AW,), 0.5, 3.0, ((0, 8),), jnp.float32)
    spatial_weight = scatter_about(seeds[8], (GROUPS, BLOCK, BLOCK), (4 * BLOCK) ** -0.5, 0.25, ((0, 8),))
    spatial_bias = jnp.clip(1.0 + 0.18 * jax.random.normal(seeds[9], (GROUPS, BLOCK), jnp.float32), 0.1, 1.9)
    merge_weight = scatter_about(seeds[10], (AW, D), AW ** -0.5, 0.1875, ((0, 8), (1, 16)), jnp.float32)
    merge_scale = jnp.clip(jnp.exp(math.log(2.0) - 1.3862944 * jax.random.uniform(seeds[11], (D,), jnp.float32) ** levels(seeds[11], (D,), ((0, 16),), -0.2, 0.2)), 0.5, 2.0)
    channel_gain = jnp.clip(1.0 + 0.18 * jax.random.normal(seeds[12], (D,), jnp.float32), 0.1, 1.9)
    expand_weight = scatter_about(seeds[13], (D, FF), D ** -0.5, 0.125, ((0, 16), (1, 8)), jnp.float32)
    expand_scale = jnp.clip(jnp.exp(math.log(2.0) - 1.3862944 * jax.random.uniform(seeds[14], (FF,), jnp.float32) ** levels(seeds[14], (FF,), ((0, 8),), -0.2, 0.2)), 0.5, 2.0)
    reduce_weight = scatter_about(seeds[15], (FF, D), FF ** -0.5, 0.0625, ((0, 8), (1, 16)), jnp.float32)
    reduce_scale = jnp.clip(jnp.exp(math.log(2.0) - 1.3862944 * jax.random.uniform(seeds[16], (D,), jnp.float32) ** levels(seeds[16], (D,), ((0, 16),), -0.2, 0.2)), 0.5, 2.0)
    return {"tokens": tokens, "mixer_gain": mixer_gain, "direct_weight": direct_weight, "direct_scale": direct_scale, "value_weight": value_weight, "value_scale": value_scale, "value_gain": value_gain, "value_shift": value_shift, "spatial_weight": spatial_weight, "spatial_bias": spatial_bias, "merge_weight": merge_weight, "merge_scale": merge_scale, "channel_gain": channel_gain, "expand_weight": expand_weight, "expand_scale": expand_scale, "reduce_weight": reduce_weight, "reduce_scale": reduce_scale}


epsilon = 1e-06

def rms_rows(rows, gain):
    floats = rows.astype(jnp.float32)
    scaled = floats * lax.rsqrt(lax.optimization_barrier(jnp.mean(floats * floats, axis=-1, keepdims=True)) + epsilon)
    return (scaled * gain).astype(jnp.bfloat16)

def split_sum(left, right, scale, parts):
    rows = left.shape[0]
    inner = left.shape[1] // parts
    lhs = left.reshape(rows, parts, inner).astype(jnp.float32)
    rhs = right.astype(jnp.bfloat16).astype(jnp.float32).reshape(parts, inner, right.shape[1])
    terms = jnp.einsum('gtk,tkd->tgd', lhs, rhs) * scale
    terms = lax.optimization_barrier(terms.astype(jnp.bfloat16)).astype(jnp.float32)
    return lax.optimization_barrier(jnp.sum(terms, axis=0))

def reference(tokens, mixer_gain, direct_weight, direct_scale, value_weight, value_scale, value_gain, value_shift, spatial_weight, spatial_bias, merge_weight, merge_scale, channel_gain, expand_weight, expand_scale, reduce_weight, reduce_scale):
    seq_rows = TOK_DEV * N_TP

    def one_sequence(rows):
        normed = rms_rows(rows, mixer_gain)
        direct = jax.nn.gelu(jnp.dot(normed, direct_weight.astype(jnp.bfloat16), preferred_element_type=jnp.float32) * direct_scale)
        value = jax.nn.gelu(jnp.dot(normed, value_weight.astype(jnp.bfloat16), preferred_element_type=jnp.float32) * value_scale)
        total = lax.optimization_barrier(jnp.sum(value, axis=1, keepdims=True))
        squares = lax.optimization_barrier(jnp.sum(value * value, axis=1, keepdims=True))
        mean = total / AW
        var = squares / AW - mean * mean
        gated_value = ((value - mean) * lax.rsqrt(var + epsilon) * value_gain + value_shift).astype(jnp.bfloat16)
        blocks = gated_value.reshape(seq_rows // BLOCK, BLOCK, GROUPS, GDIM).astype(jnp.float32)
        mixed = jnp.einsum('gpq,nqgc->npgc', spatial_weight.astype(jnp.float32), blocks)
        mixed = mixed + jnp.transpose(spatial_bias)[None, :, :, None]
        gated = (direct * mixed.reshape(seq_rows, AW)).astype(jnp.bfloat16)
        mix = split_sum(gated, merge_weight, merge_scale, N_TP)
        middle = (rows.astype(jnp.float32) + mix).astype(jnp.bfloat16)
        normed_mid = rms_rows(middle, channel_gain)
        upper = jnp.dot(normed_mid, expand_weight.astype(jnp.bfloat16), preferred_element_type=jnp.float32) * expand_scale
        hidden = jnp.square(jax.nn.relu(upper)).astype(jnp.bfloat16)
        lower = split_sum(hidden, reduce_weight, reduce_scale, N_TP)
        return (middle.astype(jnp.float32) + lower).astype(jnp.bfloat16)
    grouped = tokens.reshape(-1, seq_rows, D)
    return lax.map(one_sequence, grouped).reshape(tokens.shape)
```

```python
import jax
import jax.numpy as jnp
from jax import lax
from jax.experimental import pallas as pl
from jax.experimental.pallas import tpu as pltpu
from jax.sharding import Mesh
from jax.sharding import PartitionSpec as P

ALL = ("rep", "z", "x", "y", "core")
FS = ("z", "x")
TP = ("y", "core")
ZRING = ("rep", "z")
EPS = 1e-06
BF = jnp.bfloat16
F32 = jnp.float32
T = 128
HALF = T // 2
D = 2048
AW = 1024
FF_DEV = 1024


def shift(x, axis, by):
    n = 8 if axis == ZRING else lax.axis_size(axis)
    return lax.ppermute(x, axis, [(i, (i + by) % n) for i in range(n)])


def swap(x):
    return lax.ppermute(x, "core", [(0, 1), (1, 0)])


def others(x, axis):
    return shift(x, axis, -1), shift(x, axis, 2), shift(x, axis, 1)


def gelu(x):
    return 0.5 * x * (1.0 + jnp.tanh(0.7978845608028654 * (x + 0.044715 * x * x * x)))


VM = pl.BlockSpec(memory_space=pltpu.VMEM)
SM = pl.BlockSpec(memory_space=pltpu.SMEM)
HB = pl.BlockSpec(memory_space=pl.ANY)


def call(kernel, outs, inputs, specs, scratch, name):
    return pl.pallas_call(
        kernel,
        out_shape=[jax.ShapeDtypeStruct(s, d) for s, d in outs],
        in_specs=specs,
        out_specs=[VM] * len(outs),
        scratch_shapes=scratch,
        compiler_params=pltpu.CompilerParams(vmem_limit_bytes=56 * 1024 * 1024),
        name=name,
    )(*inputs)


def rms(floats, gain):
    return floats * lax.rsqrt(jnp.mean(floats * floats, axis=-1, keepdims=True) + EPS) * gain


def norm_kernel(tokens, gain, low, high):
    normed = rms(tokens[...].astype(F32), gain[...]).astype(BF)
    low[...] = normed[:HALF]
    high[...] = normed[HALF:]


def copies(pairs, sem):
    started = [pltpu.make_async_copy(src, dst, sem) for src, dst in pairs]
    for c in started:
        c.start()
    return started


def finish(started):
    for c in started:
        c.wait()


def place_of(idx, zr, xr):
    return lax.rem(idx[0] + zr, 4) * 4 + lax.rem(idx[1] + xr, 4)


def aligned(x):
    return pl.multiple_of(x * T, T)


def dv_kernel(groups, idx, own, partner, *rest):
    tokens = rest[: 2 * groups]
    outs = rest[2 * groups : 3 * groups]
    weight, sem = rest[3 * groups :]
    pairs = []
    for q, source in enumerate((own, partner)):
        for zr in range(4):
            for xr in range(4):
                row = aligned(place_of(idx, zr, xr))
                pairs.append((source.at[zr, xr], weight.at[pl.ds(row, T), q * T : (q + 1) * T]))
                pairs.append(
                    (source.at[4 + xr, zr], weight.at[pl.ds(row, T), (2 + q) * T : (3 + q) * T])
                )
    started = copies(pairs, sem)
    rows = jnp.concatenate([t[...] for t in tokens], axis=0)
    finish(started)
    full = gelu(jnp.dot(rows, weight[...], preferred_element_type=F32)).astype(BF)
    for g, out in enumerate(outs):
        out[...] = full[g * T : (g + 1) * T]


def dv(idx, own, partner, tokens, name):
    groups = len(tokens) // 2
    return call(
        lambda *refs: dv_kernel(groups, *refs),
        [((T, 4 * T), BF)] * groups,
        (idx, own, partner, *tokens),
        [SM, HB, HB] + [VM] * len(tokens),
        [pltpu.VMEM((D, 4 * T), BF), pltpu.SemaphoreType.DMA(())],
        name,
    )


def mixer_kernel(idx, tokens, gain, v0, v1, v2, v3, pack_own, pack_partner, *rest):
    merges = rest[:16]
    middle, low, high = rest[16:19]
    weight, gated, sem = rest[19:]
    pairs = []
    for q in range(2):
        first = merges[8 * q : 8 * q + 4]
        second = merges[8 * q + 4 : 8 * q + 8]
        for zr in range(4):
            for xr in range(4):
                col = aligned(place_of(idx, zr, xr))
                for r in range(4):
                    source = first[zr].at[xr] if r < 2 else second[xr].at[zr]
                    pairs.append(
                        (
                            source.at[(r % 2) * T : (r % 2 + 1) * T],
                            weight.at[(2 * r + q) * T : (2 * r + q + 1) * T, pl.ds(col, T)],
                        )
                    )
    started = copies(pairs, sem)
    parts = (v0, v1, v2, v3)
    total = jnp.zeros((T, 1), F32)
    squares = jnp.zeros((T, 1), F32)
    for r in range(4):
        value = parts[r][:, 2 * T :].astype(F32)
        total += jnp.sum(value, axis=1, keepdims=True)
        squares += jnp.sum(value * value, axis=1, keepdims=True)
    mean = total * (1.0 / AW)
    var = squares * (1.0 / AW) - mean * mean
    scale = lax.rsqrt(var + EPS)
    lane = lax.broadcasted_iota(jnp.int32, (T, T), 1)
    for r in range(4):
        for q, pack in enumerate((pack_own, pack_partner)):
            gains = pack[r, 3 * T : 3 * T + 16].astype(F32)
            gain_row = gains[0:1] + gains[1:2]
            shift_row = gains[2:3] + gains[3:4]
            bias = pack[r, 2 * T : 3 * T].astype(F32)
            bias_low = bias[:, 0:1] + bias[:, 1:2]
            bias_high = bias[:, 2:3] + bias[:, 3:4]
            value = parts[r][:, (2 + q) * T : (3 + q) * T].astype(F32)
            ready = ((value - mean) * scale * gain_row + shift_row).astype(BF)
            left = jnp.dot(pack[r, 0:T], ready, preferred_element_type=F32) + bias_low
            right = jnp.dot(pack[r, T : 2 * T], ready, preferred_element_type=F32) + bias_high
            mixed = jnp.where(lane < T // 2, left, right)
            direct = parts[r][:, q * T : (q + 1) * T].astype(F32)
            at = (2 * r + q) * T
            gated[:, at : at + T] = (direct * mixed).astype(BF)
    finish(started)
    mix = jnp.dot(gated[...], weight[...], preferred_element_type=F32)
    mid = (tokens[...].astype(F32) + mix).astype(BF)
    middle[...] = mid
    normed = rms(mid.astype(F32), gain[...]).astype(BF)
    low[...] = normed[:HALF]
    high[...] = normed[HALF:]


def ff_kernel(groups, idx, *refs):
    expands = refs[:16]
    reduces = refs[16:32]
    tokens = refs[32 : 32 + 2 * groups]
    outs = refs[32 + 2 * groups : 32 + 4 * groups]
    up, down, hidden, sem_up, sem_down = refs[32 + 4 * groups :]
    ups, downs = [], []
    for q in range(2):
        for zr in range(4):
            for xr in range(4):
                at = aligned(place_of(idx, zr, xr))
                source = expands[8 * q + 2 * zr + xr // 2].at[xr % 2]
                ups.append((source, up.at[pl.ds(at, T), q * FF_DEV : (q + 1) * FF_DEV]))
                source = reduces[8 * q + 2 * xr + zr // 2].at[zr % 2]
                downs.append((source, down.at[q * FF_DEV : (q + 1) * FF_DEV, pl.ds(at, T)]))
    ups = copies(ups, sem_up)
    downs = copies(downs, sem_down)
    rows = jnp.concatenate([t[...] for t in tokens], axis=0)
    finish(ups)
    for n in range(4):
        cols = slice(n * 512, (n + 1) * 512)
        pre = jnp.dot(rows, up[:, cols], preferred_element_type=F32)
        hidden[:, cols] = jnp.square(jnp.maximum(pre, 0.0)).astype(BF)
    finish(downs)
    for n in range(4):
        cols = slice(n * 512, (n + 1) * 512)
        part = jnp.dot(hidden[...], down[:, cols], preferred_element_type=F32).astype(BF)
        for g, out in enumerate(outs):
            out[:, cols] = part[g * HALF : (g + 1) * HALF]


def ff(idx, expands, reduces, tokens, name):
    groups = len(tokens) // 2
    return call(
        lambda *refs: ff_kernel(groups, *refs),
        [((HALF, D), BF)] * (2 * groups),
        (idx, *expands, *reduces, *tokens),
        [SM] + [HB] * 32 + [VM] * len(tokens),
        [
            pltpu.VMEM((D, 2 * FF_DEV), BF),
            pltpu.VMEM((2 * FF_DEV, D), BF),
            pltpu.VMEM((groups * T, 2 * FF_DEV), BF),
            pltpu.SemaphoreType.DMA(()),
            pltpu.SemaphoreType.DMA(()),
        ],
        name,
    )


def both_halves(x):
    high = lax.reduce_precision(x, 8, 7)
    return high.astype(BF), (x - high).astype(BF)


def gathered_small(x, first, second):
    stack = jnp.stack([x, *others(x, first)])
    return (stack, *others(stack, second))


def gathered_large(x, first, second):
    near, far, back = others(x, first)
    low, high = jnp.stack([x, near]), jnp.stack([far, back])
    low_back, high_back = shift(low, second, 1), shift(high, second, 1)
    high_next, low_next = shift(high, second, -1), shift(low, second, -1)
    low_far, high_far = shift(low_back, second, 1), shift(high_next, second, -1)
    return low, high, low_next, high_next, low_far, high_far, low_back, high_back


def row_halves_gathered(low, high):
    low_back, high_next = shift(low, "y", 1), shift(high, "y", -1)
    high_back, low_next = shift(high, "y", 1), shift(low, "y", -1)
    low_far, high_far = shift(low_back, "y", 1), shift(high_next, "y", -1)
    return (low_next, high_next), (low_far, high_far), (low_back, high_back)


def body(
    tokens,
    mixer_gain,
    direct_weight,
    direct_scale,
    value_weight,
    value_scale,
    value_gain,
    value_shift,
    spatial_weight,
    spatial_bias,
    merge_weight,
    merge_scale,
    channel_gain,
    expand_weight,
    expand_scale,
    reduce_weight,
    reduce_scale,
):
    idx = jnp.stack([lax.axis_index("z"), lax.axis_index("x")]).astype(jnp.int32)
    low, high = call(
        norm_kernel,
        [((HALF, D), BF)] * 2,
        (tokens, mixer_gain.reshape(1, D)),
        [VM, VM],
        [],
        "norm",
    )
    next_rows, far_rows, back_rows = row_halves_gathered(low, high)
    direct_half = (direct_weight * direct_scale).astype(BF)
    value_half = (value_weight * value_scale).astype(BF)
    dv_own = jnp.stack(
        [*gathered_small(direct_half, "x", ZRING), *gathered_small(value_half, ZRING, "x")]
    )
    dv_partner = swap(dv_own)

    merge_half = (merge_weight * merge_scale).astype(BF)
    merge_y = [merge_half, *others(merge_half, "y")]
    merge_own = (
        *gathered_small(jnp.concatenate(merge_y[:2]), "x", ZRING),
        *gathered_small(jnp.concatenate(merge_y[2:]), ZRING, "x"),
    )
    merge_partner = tuple(swap(m) for m in merge_own)

    gain_high, gain_low = both_halves(value_gain)
    shift_high, shift_low = both_halves(value_shift)
    bias_high, bias_low = both_halves(spatial_bias)
    bias_columns = jnp.stack([bias_high[0], bias_low[0], bias_high[1], bias_low[1]], axis=1)
    pack = jnp.concatenate(
        [
            spatial_weight.reshape(2 * T, T),
            jnp.pad(bias_columns, ((0, 0), (0, T - 4))),
            jnp.pad(jnp.stack([gain_high, gain_low, shift_high, shift_low]), ((0, 12), (0, 0))),
        ]
    )
    pack_own = jnp.stack([pack, *others(pack, "y")])
    pack_partner = swap(pack_own)

    expand_half = (expand_weight * expand_scale).astype(BF)
    reduce_half = (reduce_weight * reduce_scale).astype(BF)
    expand_own = gathered_large(expand_half, "x", ZRING)
    reduce_own = gathered_large(reduce_half, ZRING, "x")
    expands = (*expand_own, *[swap(e) for e in expand_own])
    reduces = (*reduce_own, *[swap(e) for e in reduce_own])

    (part_own,) = dv(idx, dv_own, dv_partner, (low, high), "dv_own")
    part_next, part_back = dv(idx, dv_own, dv_partner, (*next_rows, *back_rows), "dv_near")
    (part_far,) = dv(idx, dv_own, dv_partner, far_rows, "dv_far")
    from_back = shift(part_next, "y", 1)
    from_next = shift(part_back, "y", -1)
    from_far = shift(part_far, "y", 2)

    middle, low, high = call(
        mixer_kernel,
        [((T, D), BF), ((HALF, D), BF), ((HALF, D), BF)],
        (
            idx,
            tokens,
            channel_gain.reshape(1, D),
            part_own,
            from_next,
            from_far,
            from_back,
            pack_own,
            pack_partner,
            *merge_own,
            *merge_partner,
        ),
        [SM] + [VM] * 8 + [HB] * 16,
        [pltpu.VMEM((AW, D), BF), pltpu.VMEM((T, AW), BF), pltpu.SemaphoreType.DMA(())],
        "mixer",
    )
    next_rows, far_rows, back_rows = row_halves_gathered(low, high)
    far_low, far_high = ff(idx, expands, reduces, far_rows, "ff_far")
    next_low, next_high, back_low, back_high = ff(
        idx, expands, reduces, (*next_rows, *back_rows), "ff_near"
    )
    own_low, own_high = ff(idx, expands, reduces, (low, high), "ff_own")
    relay_low = shift(far_low, "y", 1)
    relay_high = shift(far_high, "y", -1)
    got_back_high = shift(next_high, "y", 1)
    got_next_low = shift(back_low, "y", -1)
    next_low = (next_low.astype(F32) + relay_low.astype(F32)).astype(BF)
    back_high = (back_high.astype(F32) + relay_high.astype(F32)).astype(BF)
    got_back_low = shift(next_low, "y", 1)
    got_next_high = shift(back_high, "y", -1)

    def total(own, one, two, mid):
        return (
            mid.astype(F32) + (own.astype(F32) + (one.astype(F32) + two.astype(F32)))
        ).astype(BF)

    return jnp.concatenate(
        [
            total(own_low, got_back_low, got_next_low, middle[:HALF]),
            total(own_high, got_back_high, got_next_high, middle[HALF:]),
        ]
    )


def solution(mesh):
    finer = Mesh(mesh.devices.reshape(2, 4, 4, 4, 2), ALL)
    in_specs = (
        P(ALL, None),
        P(),
        P(FS, TP),
        P(TP),
        P(FS, TP),
        P(TP),
        P(TP),
        P(TP),
        P(TP, None, None),
        P(TP, None),
        P(TP, FS),
        P(FS),
        P(),
        P(FS, TP),
        P(TP),
        P(TP, FS),
        P(FS),
    )
    return jax.shard_map(body, mesh=finer, in_specs=in_specs, out_specs=P(ALL, None), check_vma=False)
```

```python
import jax
import jax.numpy as jnp
from jax import lax
from jax.experimental import pallas as pl
from jax.experimental.pallas import tpu as pltpu
from jax.sharding import Mesh
from jax.sharding import PartitionSpec as P

ALL = ("rep", "z", "x", "y", "core")
FS = ("z", "x")
TP = ("y", "core")
ZRING = ("rep", "z")
EPS = 1e-06
BF = jnp.bfloat16
F32 = jnp.float32
T = 128
HALF = T // 2
D = 2048
AW = 1024
FF_DEV = 1024
K = D // T
PACK = 3 * T + 16
CHUNK = 256


def shift(x, axis, by):
    n = 8 if axis == ZRING else lax.axis_size(axis)
    return lax.ppermute(x, axis, [(i, (i + by) % n) for i in range(n)])


def swap(x):
    return lax.ppermute(x, "core", [(0, 1), (1, 0)])


def others(x, axis):
    return (shift(x, axis, -1), shift(x, axis, 2), shift(x, axis, 1))


def gelu(x):
    return 0.5 * x * (1.0 + jnp.tanh(0.7978845608028654 * (x + 0.044715 * x * x * x)))


VM = pl.BlockSpec(memory_space=pltpu.VMEM)
SM = pl.BlockSpec(memory_space=pltpu.SMEM)
HB = pl.BlockSpec(memory_space=pl.ANY)


def call(kernel, outs, inputs, specs, scratch, out_specs=None):
    return pl.pallas_call(
        kernel,
        out_shape=[jax.ShapeDtypeStruct(s, d) for s, d in outs],
        in_specs=specs,
        out_specs=out_specs or [VM] * len(outs),
        scratch_shapes=scratch,
        compiler_params=pltpu.CompilerParams(vmem_limit_bytes=56 * 1024 * 1024),
    )(*inputs)


def rms(floats, gain):
    return floats * lax.rsqrt(jnp.mean(floats * floats, axis=-1, keepdims=True) + EPS) * gain


def rows_of(first, second):
    high = first.astype(BF).astype(F32)
    other = second.astype(BF).astype(F32)
    return [high, first - high, other, second - other]


def norm_kernel(tokens, gain, spatial, value_gain, value_shift, bias, out):
    normed = rms(tokens[...].astype(F32), gain[...]).astype(BF)
    for k in range(K):
        out[k * T : (k + 1) * T] = normed[:, k * T : (k + 1) * T]
    out[D : D + 2 * T] = spatial[...]
    tall = jnp.concatenate([*rows_of(bias[0:1], bias[1:2]), jnp.zeros((T - 4, T), F32)], axis=0)
    out[D + 2 * T : D + 3 * T] = tall.T.astype(BF)
    gains = [*rows_of(value_gain[...], value_shift[...]), jnp.zeros((12, T), F32)]
    out[D + 3 * T : D + PACK] = jnp.concatenate(gains, axis=0).astype(BF)


def copies(pairs, sem):
    started = [pltpu.make_async_copy(src, dst, sem) for src, dst in pairs]
    for c in started:
        c.start()
    return started


def finish(started):
    for c in started:
        c.wait()


def place_of(idx, zr, xr):
    return lax.rem(idx[0] + zr, 4) * 4 + lax.rem(idx[1] + xr, 4)


def aligned(x):
    return pl.multiple_of(x * T, T)


def dv_kernel(idx, *refs):
    weights = refs[:8]
    sources = refs[8:12]
    outs = refs[12:16]
    pack = refs[16]
    weight, rows, sem = refs[17:]
    pairs = []
    for q in range(2):
        for zr in range(4):
            for xr in range(4):
                row = aligned(place_of(idx, zr, xr))
                dst = weight.at[pl.ds(row, T), 2 * q * T : 2 * (q + 1) * T]
                pairs.append((weights[4 * q + zr].at[xr], dst))
    for g, source in enumerate(sources):
        for k in range(K):
            dst = rows.at[g * T : (g + 1) * T, k * T : (k + 1) * T]
            pairs.append((source.at[k * T : (k + 1) * T], dst))
        pairs.append((source.at[D : D + PACK], pack.at[g]))
    finish(copies(pairs, sem))
    for g, out in enumerate(outs):
        part = jnp.dot(rows[g * T : (g + 1) * T], weight[...], preferred_element_type=F32)
        out[...] = gelu(part).astype(BF)


def mixer_kernel(idx, tokens, gain, v0, v1, v2, v3, pack_own, pack_partner, *rest):
    merges = rest[:8]
    middle, normed = rest[8:10]
    weight, gated, sem = rest[10:]
    pairs = []
    for q in range(2):
        for zr in range(4):
            for xr in range(4):
                col = aligned(place_of(idx, zr, xr))
                for r in range(4):
                    at = (2 * r + q) * T
                    dst = weight.at[at : at + T, pl.ds(col, T)]
                    pairs.append((merges[4 * q + xr].at[zr, r * T : (r + 1) * T], dst))
    started = copies(pairs, sem)
    parts = (v0, v1, v2, v3)
    columns = [parts[r][:, (2 * q + 1) * T : (2 * q + 2) * T] for r in range(4) for q in range(2)]
    total = jnp.zeros((T, 1), F32)
    squares = jnp.zeros((T, 1), F32)
    for column in columns:
        value = column.astype(F32)
        total += jnp.sum(value, axis=1, keepdims=True)
        squares += jnp.sum(value * value, axis=1, keepdims=True)
    mean = total * (1.0 / AW)
    var = squares * (1.0 / AW) - mean * mean
    scale = lax.rsqrt(var + EPS)
    lane = lax.broadcasted_iota(jnp.int32, (T, T), 1)
    for r in range(4):
        for q, pack in enumerate((pack_own, pack_partner)):
            gains = pack[r, 3 * T : 3 * T + 16].astype(F32)
            gain_row = gains[0:1] + gains[1:2]
            shift_row = gains[2:3] + gains[3:4]
            bias = pack[r, 2 * T : 3 * T].astype(F32)
            bias_low = bias[:, 0:1] + bias[:, 1:2]
            bias_high = bias[:, 2:3] + bias[:, 3:4]
            value = columns[2 * r + q].astype(F32)
            ready = ((value - mean) * scale * gain_row + shift_row).astype(BF)
            left = jnp.dot(pack[r, 0:T], ready, preferred_element_type=F32) + bias_low
            right = jnp.dot(pack[r, T : 2 * T], ready, preferred_element_type=F32) + bias_high
            mixed = jnp.where(lane < T // 2, left, right)
            direct = parts[r][:, 2 * q * T : (2 * q + 1) * T].astype(F32)
            at = (2 * r + q) * T
            gated[:, at : at + T] = (direct * mixed).astype(BF)
    finish(started)
    mix = jnp.dot(gated[...], weight[...], preferred_element_type=F32)
    mid = (tokens[...].astype(F32) + mix).astype(BF)
    middle[...] = mid
    normed[...] = rms(mid.astype(F32), gain[...]).astype(BF)


def halves_of(parts, zr):
    own, near, far_low, far_high, back = parts
    if zr == 2:
        return lambda n: (far_low, far_high)[n // 2].at[n % 2]
    return lambda n: (own, near, None, back)[zr].at[n]


def up_kernel(idx, *refs):
    out, sem = refs[10:]
    pairs = []
    for q in range(2):
        for zr in range(4):
            pick = halves_of(refs[5 * q : 5 * q + 5], zr)
            for xr in range(4):
                at = aligned(place_of(idx, zr, xr))
                pairs.append((pick(xr), out.at[pl.ds(at, T), q * FF_DEV : (q + 1) * FF_DEV]))
    finish(copies(pairs, sem))


def down_kernel(idx, *refs):
    out, sem = refs[10:]
    pairs = []
    for q in range(2):
        for xr in range(4):
            pick = halves_of(refs[5 * q : 5 * q + 5], xr)
            for zr in range(4):
                at = aligned(place_of(idx, zr, xr))
                pairs.append((pick(zr), out.at[q * FF_DEV : (q + 1) * FF_DEV, pl.ds(at, T)]))
    finish(copies(pairs, sem))


def ff_kernel(groups, up, down, *refs):
    tokens = refs[:groups]
    outs = refs[groups : 2 * groups]
    rows, hidden = refs[2 * groups :]
    for g, t in enumerate(tokens):
        rows[g * T : (g + 1) * T] = t[...]

    @pl.loop(0, D // CHUNK)
    def _(n):
        cols = pl.ds(pl.multiple_of(n * CHUNK, CHUNK), CHUNK)
        pre = jnp.dot(rows[...], up[:, cols], preferred_element_type=F32)
        hidden[:, cols] = jnp.square(jnp.maximum(pre, 0.0)).astype(BF)

    @pl.loop(0, D // CHUNK)
    def _(n):
        cols = pl.ds(pl.multiple_of(n * CHUNK, CHUNK), CHUNK)
        part = jnp.dot(hidden[...], down[:, cols], preferred_element_type=F32).astype(BF)
        for g, out in enumerate(outs):
            out[:, cols] = part[g * T : (g + 1) * T]


def ff(up, down, tokens):
    groups = len(tokens)
    return call(
        lambda *refs: ff_kernel(groups, *refs),
        [((T, D), BF)] * groups,
        (up, down, *tokens),
        [VM] * (2 + groups),
        [pltpu.VMEM((groups * T, D), BF), pltpu.VMEM((groups * T, D), BF)],
    )


def gathered_small(x, first, second):
    stack = jnp.stack([x, *others(x, first)])
    return (stack, *others(stack, second))


def gathered_large(x, first, second):
    stack = jnp.stack([x, *others(x, first)])
    near = shift(stack, second, -1)
    back = shift(stack, second, 1)
    far_low = shift(back[:2], second, 1)
    far_high = shift(near[2:], second, -1)
    return stack, near, far_low, far_high, back


def swapped(arrays):
    return tuple(swap(a) for a in arrays)


def layer(
    tokens,
    mixer_gain,
    direct_weight,
    direct_scale,
    value_weight,
    value_scale,
    value_gain,
    value_shift,
    spatial_weight,
    spatial_bias,
    merge_weight,
    merge_scale,
    channel_gain,
    expand_weight,
    expand_scale,
    reduce_weight,
    reduce_scale,
):
    idx = jnp.stack([lax.axis_index("z"), lax.axis_index("x")]).astype(jnp.int32)
    merge_half = (merge_weight * merge_scale).astype(BF)
    merge_y = jnp.concatenate([merge_half, *others(merge_half, "y")])
    dv_half = jnp.concatenate(
        [(direct_weight * direct_scale).astype(BF), (value_weight * value_scale).astype(BF)], axis=1
    )
    dv_own = gathered_small(dv_half, "x", ZRING)
    (normed,) = call(
        norm_kernel,
        [((D + PACK, T), BF)],
        (
            tokens,
            mixer_gain.reshape(1, D),
            spatial_weight.reshape(2 * T, T),
            value_gain.reshape(1, T),
            value_shift.reshape(1, T),
            spatial_bias,
        ),
        [VM] * 6,
        [],
    )
    near_rows, far_rows, back_rows = others(normed, "y")
    dv_partner = swapped(dv_own)
    merge_own = gathered_small(merge_y, ZRING, "x")
    merge_partner = swapped(merge_own)
    expand_own = gathered_large((expand_weight * expand_scale).astype(BF), "x", ZRING)
    reduce_own = gathered_large((reduce_weight * reduce_scale).astype(BF), ZRING, "x")
    expand_partner = swapped(expand_own)
    reduce_partner = swapped(reduce_own)

    part_own, part_near, part_far, part_back, pack_own = call(
        dv_kernel,
        [((T, 4 * T), BF)] * 4 + [((4, PACK, T), BF)],
        (idx, *dv_own, *dv_partner, normed, near_rows, far_rows, back_rows),
        [SM] + [HB] * 12,
        [
            pltpu.VMEM((D, 4 * T), BF),
            pltpu.VMEM((4 * T, D), BF),
            pltpu.SemaphoreType.DMA(()),
        ],
        [VM] * 4 + [HB],
    )
    pack_partner = swap(pack_own)
    from_back = shift(part_near, "y", 1)
    from_near = shift(part_back, "y", -1)
    from_far = shift(part_far, "y", 2)

    middle, normed = call(
        mixer_kernel,
        [((T, D), BF), ((T, D), BF)],
        (
            idx,
            tokens,
            channel_gain.reshape(1, D),
            part_own,
            from_near,
            from_far,
            from_back,
            pack_own,
            pack_partner,
            *merge_own,
            *merge_partner,
        ),
        [SM] + [VM] * 8 + [HB] * 8,
        [pltpu.VMEM((AW, D), BF), pltpu.VMEM((T, AW), BF), pltpu.SemaphoreType.DMA(())],
    )
    near_rows, far_rows, back_rows = others(normed, "y")
    dma = [pltpu.SemaphoreType.DMA(())]
    (up,) = call(
        up_kernel,
        [((D, 2 * FF_DEV), BF)],
        (idx, *expand_own, *expand_partner),
        [SM] + [HB] * 10,
        dma,
    )
    (down,) = call(
        down_kernel,
        [((2 * FF_DEV, D), BF)],
        (idx, *reduce_own, *reduce_partner),
        [SM] + [HB] * 10,
        dma,
    )
    (far,) = ff(up, down, (far_rows,))
    near, back = ff(up, down, (near_rows, back_rows))
    (own,) = ff(up, down, (normed,))
    relay_low = shift(far[:HALF], "y", 1)
    relay_high = shift(far[HALF:], "y", -1)

    def plus(x, relayed):
        return (x.astype(F32) + relayed.astype(F32)).astype(BF)

    near = jnp.concatenate([plus(near[:HALF], relay_low), near[HALF:]])
    back = jnp.concatenate([back[:HALF], plus(back[HALF:], relay_high)])
    got_back = shift(near, "y", 1)
    got_near = shift(back, "y", -1)
    lower = own.astype(F32) + (got_back.astype(F32) + got_near.astype(F32))
    return (middle.astype(F32) + lower).astype(BF)


def solution(mesh):
    finer = Mesh(mesh.devices.reshape(2, 4, 4, 4, 2), ALL)
    in_specs = (
        P(ALL, None),
        P(),
        P(FS, TP),
        P(TP),
        P(FS, TP),
        P(TP),
        P(TP),
        P(TP),
        P(TP, None, None),
        P(TP, None),
        P(TP, FS),
        P(FS),
        P(),
        P(FS, TP),
        P(TP),
        P(TP, FS),
        P(FS),
    )
    return jax.shard_map(layer, mesh=finer, in_specs=in_specs, out_specs=P(ALL, None), check_vma=False)
```

```python
import jax
import jax.numpy as jnp
from jax import lax
from jax.experimental import pallas as pl
from jax.experimental.pallas import tpu as pltpu
from jax.sharding import Mesh
from jax.sharding import PartitionSpec as P

ALL = ("rep", "z", "x", "y", "core")
FS = ("z", "x")
TP = ("y", "core")
ZRING = ("rep", "z")
EPS = 1e-06
BF = jnp.bfloat16
F32 = jnp.float32
T = 128
HALF = T // 2
D = 2048
AW = 1024
FF_DEV = 1024
K = D // T
PACK = 3 * T + 16
CHUNK = 256


def shift(x, axis, by):
    n = 8 if axis == ZRING else lax.axis_size(axis)
    pairs = [(i, (i + by) % n) for i in range(n)]
    if axis == ZRING and by == 2:
        pairs = [(i, (i + (2 if i % 2 == 0 else -2)) % n) for i in range(n)]
    return lax.ppermute(x, axis, pairs)


def swap(x):
    return lax.ppermute(x, "core", [(0, 1), (1, 0)])


def others(x, axis):
    return (shift(x, axis, -1), shift(x, axis, 2), shift(x, axis, 1))


def gelu(x):
    return 0.5 * x * (1.0 + jnp.tanh(0.7978845608028654 * (x + 0.044715 * x * x * x)))


VM = pl.BlockSpec(memory_space=pltpu.VMEM)
SM = pl.BlockSpec(memory_space=pltpu.SMEM)
HB = pl.BlockSpec(memory_space=pl.ANY)


def call(kernel, outs, inputs, specs, scratch, out_specs=None, vmem=8):
    return pl.pallas_call(
        kernel,
        out_shape=[jax.ShapeDtypeStruct(s, d) for s, d in outs],
        in_specs=specs,
        out_specs=out_specs or [VM] * len(outs),
        scratch_shapes=scratch,
        compiler_params=pltpu.CompilerParams(vmem_limit_bytes=vmem * 1024 * 1024),
    )(*inputs)


def rms(floats, gain):
    return floats * lax.rsqrt(jnp.mean(floats * floats, axis=-1, keepdims=True) + EPS) * gain


def rows_of(first, second):
    high = first.astype(BF).astype(F32)
    other = second.astype(BF).astype(F32)
    return [high, first - high, other, second - other]


def norm_kernel(tokens, gain, spatial, value_gain, value_shift, bias, out):
    normed = rms(tokens[...].astype(F32), gain[...]).astype(BF)
    for k in range(K):
        out[k * T : (k + 1) * T] = normed[:, k * T : (k + 1) * T]
    out[D : D + 2 * T] = spatial[...]
    tall = jnp.concatenate([*rows_of(bias[0:1], bias[1:2]), jnp.zeros((T - 4, T), F32)], axis=0)
    out[D + 2 * T : D + 3 * T] = tall.T.astype(BF)
    gains = [*rows_of(value_gain[...], value_shift[...]), jnp.zeros((12, T), F32)]
    out[D + 3 * T : D + PACK] = jnp.concatenate(gains, axis=0).astype(BF)


def copies(pairs, sem):
    started = [pltpu.make_async_copy(src, dst, sem) for src, dst in pairs]
    for c in started:
        c.start()
    return started


def finish(started):
    for c in started:
        c.wait()


def place_of(idx, zr, xr):
    return lax.rem(idx[0] + zr, 4) * 4 + lax.rem(idx[1] + xr, 4)


def aligned(x):
    return pl.multiple_of(x * T, T)


def dv_kernel(idx, *refs):
    weights = refs[:8]
    sources = refs[8:12]
    outs = refs[12:16]
    pack = refs[16]
    weight, rows, sem = refs[17:]
    pairs = []
    for q in range(2):
        for zr in range(4):
            for xr in range(4):
                row = aligned(place_of(idx, zr, xr))
                dst = weight.at[pl.ds(row, T), 2 * q * T : 2 * (q + 1) * T]
                pairs.append((weights[4 * q + zr].at[xr], dst))
    for g, source in enumerate(sources):
        for k in range(K):
            dst = rows.at[g * T : (g + 1) * T, k * T : (k + 1) * T]
            pairs.append((source.at[k * T : (k + 1) * T], dst))
        pairs.append((source.at[D : D + PACK], pack.at[g]))
    finish(copies(pairs, sem))
    full = gelu(jnp.dot(rows[...], weight[...], preferred_element_type=F32)).astype(BF)
    for g, out in enumerate(outs):
        out[...] = full[g * T : (g + 1) * T]


def mixer_kernel(idx, tokens, gain, v0, v1, v2, v3, pack_own, pack_partner, *rest):
    merges = rest[:8]
    middle, normed = rest[8:10]
    weight, gated, sem = rest[10:]
    pairs = []
    for q in range(2):
        for zr in range(4):
            for xr in range(4):
                col = aligned(place_of(idx, zr, xr))
                for r in range(4):
                    at = (2 * r + q) * T
                    dst = weight.at[at : at + T, pl.ds(col, T)]
                    pairs.append((merges[4 * q + xr].at[zr, r * T : (r + 1) * T], dst))
    started = copies(pairs, sem)
    parts = (v0, v1, v2, v3)
    columns = [parts[r][:, (2 * q + 1) * T : (2 * q + 2) * T] for r in range(4) for q in range(2)]
    total = jnp.zeros((T, 1), F32)
    squares = jnp.zeros((T, 1), F32)
    for column in columns:
        value = column.astype(F32)
        total += jnp.sum(value, axis=1, keepdims=True)
        squares += jnp.sum(value * value, axis=1, keepdims=True)
    mean = total * (1.0 / AW)
    var = squares * (1.0 / AW) - mean * mean
    scale = lax.rsqrt(var + EPS)
    lane = lax.broadcasted_iota(jnp.int32, (T, T), 1)
    for r in range(4):
        for q, pack in enumerate((pack_own, pack_partner)):
            gains = pack[r, 3 * T : 3 * T + 16].astype(F32)
            gain_row = gains[0:1] + gains[1:2]
            shift_row = gains[2:3] + gains[3:4]
            bias = pack[r, 2 * T : 3 * T].astype(F32)
            bias_low = bias[:, 0:1] + bias[:, 1:2]
            bias_high = bias[:, 2:3] + bias[:, 3:4]
            value = columns[2 * r + q].astype(F32)
            ready = ((value - mean) * scale * gain_row + shift_row).astype(BF)
            left = jnp.dot(pack[r, 0:T], ready, preferred_element_type=F32) + bias_low
            right = jnp.dot(pack[r, T : 2 * T], ready, preferred_element_type=F32) + bias_high
            mixed = jnp.where(lane < T // 2, left, right)
            direct = parts[r][:, 2 * q * T : (2 * q + 1) * T].astype(F32)
            at = (2 * r + q) * T
            gated[:, at : at + T] = (direct * mixed).astype(BF)
    finish(started)
    mix = jnp.dot(gated[...], weight[...], preferred_element_type=F32)
    mid = (tokens[...].astype(F32) + mix).astype(BF)
    middle[...] = mid
    normed[...] = rms(mid.astype(F32), gain[...]).astype(BF)


def halves_of(parts, zr):
    own, near, far_low, far_high, back = parts
    if zr == 2:
        return lambda n: (far_low, far_high)[n // 2].at[n % 2]
    return lambda n: (own, near, None, back)[zr].at[n]


def up_kernel(idx, *refs):
    out, sem = refs[10:]
    pairs = []
    for q in range(2):
        for zr in range(4):
            pick = halves_of(refs[5 * q : 5 * q + 5], zr)
            for xr in range(4):
                at = aligned(place_of(idx, zr, xr))
                pairs.append((pick(xr), out.at[pl.ds(at, T), q * FF_DEV : (q + 1) * FF_DEV]))
    finish(copies(pairs, sem))


def down_kernel(idx, *refs):
    out, sem = refs[10:]
    pairs = []
    for q in range(2):
        for xr in range(4):
            pick = halves_of(refs[5 * q : 5 * q + 5], xr)
            for zr in range(4):
                at = aligned(place_of(idx, zr, xr))
                pairs.append((pick(zr), out.at[q * FF_DEV : (q + 1) * FF_DEV, pl.ds(at, T)]))
    finish(copies(pairs, sem))


def ff_kernel(groups, up, down, *refs):
    tokens = refs[:groups]
    outs = refs[groups : 2 * groups]
    rows, hidden = refs[2 * groups :]
    for g, t in enumerate(tokens):
        rows[g * T : (g + 1) * T] = t[...]

    @pl.loop(0, D // CHUNK)
    def _(n):
        cols = pl.ds(pl.multiple_of(n * CHUNK, CHUNK), CHUNK)
        pre = jnp.dot(rows[...], up[:, cols], preferred_element_type=F32)
        hidden[:, cols] = jnp.square(jnp.maximum(pre, 0.0)).astype(BF)

    @pl.loop(0, D // CHUNK)
    def _(n):
        cols = pl.ds(pl.multiple_of(n * CHUNK, CHUNK), CHUNK)
        part = jnp.dot(hidden[...], down[:, cols], preferred_element_type=F32).astype(BF)
        for g, out in enumerate(outs):
            out[:, cols] = part[g * T : (g + 1) * T]


def ff(up, down, tokens):
    groups = len(tokens)
    return call(
        lambda *refs: ff_kernel(groups, *refs),
        [((T, D), BF)] * groups,
        (up, down, *tokens),
        [VM] * (2 + groups),
        [pltpu.VMEM((groups * T, D), BF), pltpu.VMEM((groups * T, D), BF)],
    )


def gathered_small(x, first, second):
    stack = jnp.stack([x, *others(x, first)])
    return (stack, *others(stack, second))


def gathered_large(x, first, second):
    stack = jnp.stack([x, *others(x, first)])
    near = shift(stack, second, -1)
    back = shift(stack, second, 1)
    far_low = shift(back[:2], second, 1)
    far_high = shift(near[2:], second, -1)
    return stack, near, far_low, far_high, back


def swapped(arrays):
    return tuple(swap(a) for a in arrays)


def layer(
    tokens,
    mixer_gain,
    direct_weight,
    direct_scale,
    value_weight,
    value_scale,
    value_gain,
    value_shift,
    spatial_weight,
    spatial_bias,
    merge_weight,
    merge_scale,
    channel_gain,
    expand_weight,
    expand_scale,
    reduce_weight,
    reduce_scale,
):
    idx = jnp.stack([lax.axis_index("z"), lax.axis_index("x")]).astype(jnp.int32)
    merge_half = (merge_weight * merge_scale).astype(BF)
    merge_y = jnp.concatenate([merge_half, *others(merge_half, "y")])
    dv_half = jnp.concatenate(
        [(direct_weight * direct_scale).astype(BF), (value_weight * value_scale).astype(BF)], axis=1
    )
    dv_own = gathered_small(dv_half, "x", ZRING)
    (normed,) = call(
        norm_kernel,
        [((D + PACK, T), BF)],
        (
            tokens,
            mixer_gain.reshape(1, D),
            spatial_weight.reshape(2 * T, T),
            value_gain.reshape(1, T),
            value_shift.reshape(1, T),
            spatial_bias,
        ),
        [VM] * 6,
        [],
    )
    near_rows, far_rows, back_rows = others(normed, "y")
    expand_weight, reduce_weight, _ = lax.optimization_barrier((expand_weight, reduce_weight, normed))
    dv_partner = swapped(dv_own)
    merge_own = gathered_small(merge_y, ZRING, "x")
    merge_partner = swapped(merge_own)
    expand_own = gathered_large((expand_weight * expand_scale).astype(BF), "x", ZRING)
    reduce_own = gathered_large((reduce_weight * reduce_scale).astype(BF), ZRING, "x")
    expand_partner = swapped(expand_own)
    reduce_partner = swapped(reduce_own)

    part_own, part_near, part_far, part_back, pack_own = call(
        dv_kernel,
        [((T, 4 * T), BF)] * 4 + [((4, PACK, T), BF)],
        (idx, *dv_own, *dv_partner, normed, near_rows, far_rows, back_rows),
        [SM] + [HB] * 12,
        [
            pltpu.VMEM((D, 4 * T), BF),
            pltpu.VMEM((4 * T, D), BF),
            pltpu.SemaphoreType.DMA(()),
        ],
        [VM] * 4 + [HB],
        16,
    )
    pack_partner = swap(pack_own)
    from_back = shift(part_near, "y", 1)
    from_near = shift(part_back, "y", -1)
    from_far = shift(part_far, "y", 2)

    middle, normed = call(
        mixer_kernel,
        [((T, D), BF), ((T, D), BF)],
        (
            idx,
            tokens,
            channel_gain.reshape(1, D),
            part_own,
            from_near,
            from_far,
            from_back,
            pack_own,
            pack_partner,
            *merge_own,
            *merge_partner,
        ),
        [SM] + [VM] * 8 + [HB] * 8,
        [pltpu.VMEM((AW, D), BF), pltpu.VMEM((T, AW), BF), pltpu.SemaphoreType.DMA(())],
        None,
        16,
    )
    near_rows, far_rows, back_rows = others(normed, "y")
    dma = [pltpu.SemaphoreType.DMA(())]
    (up,) = call(
        up_kernel,
        [((D, 2 * FF_DEV), BF)],
        (idx, *expand_own, *expand_partner),
        [SM] + [HB] * 10,
        dma,
    )
    (down,) = call(
        down_kernel,
        [((2 * FF_DEV, D), BF)],
        (idx, *reduce_own, *reduce_partner),
        [SM] + [HB] * 10,
        dma,
    )
    (far,) = ff(up, down, (far_rows,))
    near, back = ff(up, down, (near_rows, back_rows))
    (own,) = ff(up, down, (normed,))
    relay_low = shift(far[:HALF], "y", 1)
    relay_high = shift(far[HALF:], "y", -1)

    def plus(x, relayed):
        return (x.astype(F32) + relayed.astype(F32)).astype(BF)

    near = jnp.concatenate([plus(near[:HALF], relay_low), near[HALF:]])
    back = jnp.concatenate([back[:HALF], plus(back[HALF:], relay_high)])
    got_back = shift(near, "y", 1)
    got_near = shift(back, "y", -1)
    lower = own.astype(F32) + (got_back.astype(F32) + got_near.astype(F32))
    return (middle.astype(F32) + lower).astype(BF)


def solution(mesh):
    finer = Mesh(mesh.devices.reshape(2, 4, 4, 4, 2), ALL)
    in_specs = (
        P(ALL, None),
        P(),
        P(FS, TP),
        P(TP),
        P(FS, TP),
        P(TP),
        P(TP),
        P(TP),
        P(TP, None, None),
        P(TP, None),
        P(TP, FS),
        P(FS),
        P(),
        P(FS, TP),
        P(TP),
        P(TP, FS),
        P(FS),
    )
    return jax.shard_map(layer, mesh=finer, in_specs=in_specs, out_specs=P(ALL, None), check_vma=False)
```

```python
import jax
import jax.numpy as jnp
from jax import lax
from jax.experimental import pallas as pl
from jax.experimental.pallas import tpu as pltpu
from jax.sharding import Mesh
from jax.sharding import PartitionSpec as P

ALL = ("rep", "z", "x", "y", "core")
FS = ("z", "x")
TP = ("y", "core")
ZRING = ("rep", "z")
EPS = 1e-06
BF = jnp.bfloat16
F32 = jnp.float32
T = 128
HALF = T // 2
D = 2048
AW = 1024
FF_DEV = 1024
K = D // T
PACK = 3 * T + 16
CHUNK = 512


def shift(x, axis, by):
    n = 8 if axis == ZRING else lax.axis_size(axis)
    pairs = [(i, (i + by) % n) for i in range(n)]
    if axis == ZRING and by == 2:
        pairs = [(i, (i + (2 if i % 2 == 0 else -2)) % n) for i in range(n)]
    return lax.ppermute(x, axis, pairs)


def swap(x):
    return lax.ppermute(x, "core", [(0, 1), (1, 0)])


def others(x, axis):
    return (shift(x, axis, -1), shift(x, axis, 2), shift(x, axis, 1))


def gelu(x):
    return 0.5 * x * (1.0 + jnp.tanh(0.7978845608028654 * (x + 0.044715 * x * x * x)))


VM = pl.BlockSpec(memory_space=pltpu.VMEM)
SM = pl.BlockSpec(memory_space=pltpu.SMEM)
HB = pl.BlockSpec(memory_space=pl.ANY)
RAW = pl.BlockSpec(memory_space=pltpu.HBM)


def call(kernel, outs, inputs, specs, scratch, out_specs=None, vmem=8):
    return pl.pallas_call(
        kernel,
        out_shape=[jax.ShapeDtypeStruct(s, d) for s, d in outs],
        in_specs=specs,
        out_specs=out_specs or [VM] * len(outs),
        scratch_shapes=scratch,
        compiler_params=pltpu.CompilerParams(vmem_limit_bytes=vmem * 1024 * 1024),
    )(*inputs)


def rms(floats, gain):
    return floats * lax.rsqrt(jnp.mean(floats * floats, axis=-1, keepdims=True) + EPS) * gain


def rows_of(first, second):
    high = first.astype(BF).astype(F32)
    other = second.astype(BF).astype(F32)
    return [high, first - high, other, second - other]


def copies(pairs, sem):
    started = [pltpu.make_async_copy(src, dst, sem) for src, dst in pairs]
    for c in started:
        c.start()
    return started


def finish(started):
    for c in started:
        c.wait()


def loaded(sources, buffers, sem):
    finish(copies(list(zip(sources, buffers)), sem))


def norm_kernel(*refs):
    sources, out, buffers, sem = refs[:6], refs[6], refs[7:13], refs[13]
    loaded(sources, buffers, sem)
    tokens, gain, spatial, value_gain, value_shift, bias = buffers
    normed = rms(tokens[...].astype(F32), gain[...]).astype(BF)
    for k in range(K):
        out[k * T : (k + 1) * T] = normed[:, k * T : (k + 1) * T]
    out[D : D + 2 * T] = spatial[...]
    tall = jnp.concatenate([*rows_of(bias[0:1], bias[1:2]), jnp.zeros((T - 4, T), F32)], axis=0)
    out[D + 2 * T : D + 3 * T] = tall.T.astype(BF)
    gains = [*rows_of(value_gain[...], value_shift[...]), jnp.zeros((12, T), F32)]
    out[D + 3 * T : D + PACK] = jnp.concatenate(gains, axis=0).astype(BF)


def columns_kernel(*refs):
    sources, out, buffers, sem = refs[:6], refs[6], refs[7:13], refs[13]
    loaded(sources, buffers, sem)
    at = 0
    for weight, scale in zip(buffers[0::2], buffers[1::2]):
        width = weight.shape[1]
        out[:, at : at + width] = (weight[...] * scale[...]).astype(BF)
        at += width


def merge_kernel(*refs):
    sources, out, buffers, sem = refs[:2], refs[2], refs[3:5], refs[5]
    loaded(sources, buffers, sem)
    out[...] = (buffers[0][...] * buffers[1][...]).astype(BF)


def rows_kernel(m0, m1, m2, m3, weight, scale, out, weight_buffer, scale_buffer, sem):
    started = copies([(weight, weight_buffer), (scale, scale_buffer)], sem)
    for r, part in enumerate((m0, m1, m2, m3)):
        out[r * T : (r + 1) * T] = part[...]
    finish(started)
    out[4 * T :] = (weight_buffer[...] * scale_buffer[...]).astype(BF)


def split_columns_kernel(c0, c1, c2, c3, first, second):
    for n, part in enumerate((c0, c1, c2, c3)):
        first[n] = part[:, : first.shape[2]]
        second[n] = part[:, first.shape[2] :]


def split_rows_kernel(r0, r1, r2, r3, first, second):
    for n, part in enumerate((r0, r1, r2, r3)):
        first[n] = part[: first.shape[1]]
        second[n] = part[first.shape[1] :]


def plus_kernel(near, back, low, high, near_out, back_out):
    near_out[:HALF] = (near[:HALF].astype(F32) + low[...].astype(F32)).astype(BF)
    near_out[HALF:] = near[HALF:]
    back_out[:HALF] = back[:HALF]
    back_out[HALF:] = (back[HALF:].astype(F32) + high[...].astype(F32)).astype(BF)


def prepared(kernel, out, raw, ready=()):
    buffers = [pltpu.VMEM(a.shape, a.dtype) for a in raw]
    return call(
        kernel,
        [(out, BF)],
        (*ready, *[pltpu.with_memory_space_constraint(a, pltpu.HBM) for a in raw]),
        [VM] * len(ready) + [RAW] * len(raw),
        [*buffers, pltpu.SemaphoreType.DMA(())],
    )[0]


def place_of(idx, zr, xr):
    return lax.rem(idx[0] + zr, 4) * 4 + lax.rem(idx[1] + xr, 4)


def aligned(x):
    return pl.multiple_of(x * T, T)


def join_kernel(*refs):
    sources, out, sem = refs[:-2], refs[-2], refs[-1]
    pairs, at = [], 0
    for source in sources:
        pairs.append((source, out.at[at : at + source.shape[0]]))
        at += source.shape[0]
    finish(copies(pairs, sem))


def halves_kernel(near, back, low, high, sem):
    finish(copies([(back.at[:2], low), (near.at[2:], high)], sem))


def joined(arrays):
    shape = (sum(a.shape[0] for a in arrays), *arrays[0].shape[1:])
    sem = [pltpu.SemaphoreType.DMA(())]
    return call(join_kernel, [(shape, BF)], arrays, [HB] * len(arrays), sem)[0]


def dv_kernel(idx, *refs):
    weights = refs[:2]
    sources = refs[2:6]
    out, pack, weight, rows, sem = refs[6:]
    pairs = []
    for q in range(2):
        for zr in range(4):
            for xr in range(4):
                row = aligned(place_of(idx, zr, xr))
                dst = weight.at[pl.ds(row, T), 2 * q * T : 2 * (q + 1) * T]
                pairs.append((weights[q].at[4 * zr + xr], dst))
    for g, source in enumerate(sources):
        pairs.append((source.at[D : D + PACK], pack.at[g]))
    started = copies(pairs, sem)

    def block(source, g, k):
        at = pl.multiple_of(k * T, T)
        return pltpu.make_async_copy(source.at[pl.ds(at, T)], rows.at[g, :, pl.ds(at, T)], sem)

    for g, source in enumerate(sources):
        pl.loop(0, K)(lambda k: block(source, g, k).start())
    finish(started)
    for g, source in enumerate(sources):
        pl.loop(0, K)(lambda k: block(source, g, k).wait())

    @pl.loop(0, 4)
    def _(g):
        part = jnp.dot(rows[g], weight[...], preferred_element_type=F32)
        out[lax.rem(idx[2] + g, 4)] = gelu(part).astype(BF)


def mixer_kernel(idx, tokens, gain, parts, pack_own, pack_partner, *rest):
    merges = rest[:2]
    middle, normed, weight, gated, sem = rest[2:]
    pairs = []
    for q in range(2):
        for zr in range(4):
            for xr in range(4):
                col = aligned(place_of(idx, zr, xr))
                dst = weight.at[4 * q * T : 4 * (q + 1) * T, pl.ds(col, T)]
                pairs.append((merges[q].at[4 * xr + zr], dst))
    started = copies(pairs, sem)

    def moments(y, sums):
        value = [parts[y, :, (2 * q + 1) * T : (2 * q + 2) * T].astype(F32) for q in range(2)]
        total = jnp.sum(value[0] + value[1], axis=1, keepdims=True)
        squares = jnp.sum(value[0] * value[0] + value[1] * value[1], axis=1, keepdims=True)
        return sums[0] + total, sums[1] + squares

    nothing = jnp.zeros((T, 1), F32)
    total, squares = lax.fori_loop(0, 4, moments, (nothing, nothing))
    mean = total * (1.0 / AW)
    var = squares * (1.0 / AW) - mean * mean
    scale = lax.rsqrt(var + EPS)
    lane = lax.broadcasted_iota(jnp.int32, (T, T), 1)

    @pl.loop(0, 4)
    def _(r):
        y = lax.rem(idx[2] + r, 4)
        for q, pack in enumerate((pack_own, pack_partner)):
            gains = pack[r, 3 * T : 3 * T + 16].astype(F32)
            gain_row = gains[0:1] + gains[1:2]
            shift_row = gains[2:3] + gains[3:4]
            bias = pack[r, 2 * T : 3 * T].astype(F32)
            bias_low = bias[:, 0:1] + bias[:, 1:2]
            bias_high = bias[:, 2:3] + bias[:, 3:4]
            value = parts[y, :, (2 * q + 1) * T : (2 * q + 2) * T].astype(F32)
            ready = ((value - mean) * scale * gain_row + shift_row).astype(BF)
            left = jnp.dot(pack[r, 0:T], ready, preferred_element_type=F32) + bias_low
            right = jnp.dot(pack[r, T : 2 * T], ready, preferred_element_type=F32) + bias_high
            mixed = jnp.where(lane < T // 2, left, right)
            direct = parts[y, :, 2 * q * T : (2 * q + 1) * T].astype(F32)
            gated[:, pl.ds(pl.multiple_of((4 * q + r) * T, T), T)] = (direct * mixed).astype(BF)

    finish(started)

    @pl.loop(0, D // CHUNK)
    def _(n):
        cols = pl.ds(pl.multiple_of(n * CHUNK, CHUNK), CHUNK)
        mix = jnp.dot(gated[...], weight[:, cols], preferred_element_type=F32)
        middle[:, cols] = (tokens[:, cols].astype(F32) + mix).astype(BF)

    normed[...] = rms(middle[...].astype(F32), gain[...]).astype(BF)


def picked(parts, n, k):
    near, far = parts
    return far.at[k] if n == 2 else near.at[(0, 4, None, 8)[n] + k]


def up_kernel(idx, *refs):
    out, sem = refs[4:]
    pairs = []
    for q in range(2):
        for zr in range(4):
            for xr in range(4):
                at = aligned(place_of(idx, zr, xr))
                dst = out.at[pl.ds(at, T), q * FF_DEV : (q + 1) * FF_DEV]
                pairs.append((picked(refs[2 * q : 2 * q + 2], zr, xr), dst))
    finish(copies(pairs, sem))


def down_kernel(idx, *refs):
    out, sem = refs[4:]
    pairs = []
    for q in range(2):
        for zr in range(4):
            for xr in range(4):
                at = aligned(place_of(idx, zr, xr))
                dst = out.at[q * FF_DEV : (q + 1) * FF_DEV, pl.ds(at, T)]
                pairs.append((picked(refs[2 * q : 2 * q + 2], xr, zr), dst))
    finish(copies(pairs, sem))


def ff_kernel(groups, up, down, *refs):
    tokens = refs[:groups]
    outs = refs[groups:-2]
    rows, hidden = refs[-2:]
    for g, t in enumerate(tokens):
        rows[g * T : (g + 1) * T] = t[...]

    @pl.loop(0, D // CHUNK)
    def _(n):
        cols = pl.ds(pl.multiple_of(n * CHUNK, CHUNK), CHUNK)
        pre = jnp.dot(rows[...], up[:, cols], preferred_element_type=F32)
        hidden[:, cols] = jnp.square(jnp.maximum(pre, 0.0)).astype(BF)

    @pl.loop(0, D // CHUNK)
    def _(n):
        cols = pl.ds(pl.multiple_of(n * CHUNK, CHUNK), CHUNK)
        part = jnp.dot(hidden[...], down[:, cols], preferred_element_type=F32).astype(BF)
        height = outs[0].shape[0]
        for g, out in enumerate(outs):
            out[:, cols] = part[g * height : (g + 1) * height]


def ff(up, down, tokens, height=T):
    groups = len(tokens)
    return call(
        lambda *refs: ff_kernel(groups, *refs),
        [((height, D), BF)] * (groups * T // height),
        (up, down, *tokens),
        [VM] * (2 + groups),
        [pltpu.VMEM((groups * T, D), BF), pltpu.VMEM((groups * T, D), BF)],
    )


def around(stack, second):
    near = shift(stack, second, -1)
    back = shift(stack, second, 1)
    low, high = call(
        halves_kernel,
        [((2, *stack.shape[1:]), BF)] * 2,
        (near, back),
        [HB] * 2,
        [pltpu.SemaphoreType.DMA(())],
    )
    far_low = shift(low, second, 1)
    far_high = shift(high, second, -1)
    mine = (joined((stack, near, back)), joined((far_low, far_high)))
    return (*mine, *[swap(m) for m in mine])


def layer(
    tokens,
    mixer_gain,
    direct_weight,
    direct_scale,
    value_weight,
    value_scale,
    value_gain,
    value_shift,
    spatial_weight,
    spatial_bias,
    merge_weight,
    merge_scale,
    channel_gain,
    expand_weight,
    expand_scale,
    reduce_weight,
    reduce_scale,
):
    idx = jnp.stack([lax.axis_index(a) for a in ("z", "x", "y")]).astype(jnp.int32)
    row = lambda v: v.reshape(1, -1)
    merge_half = prepared(merge_kernel, (T, T), (merge_weight, row(merge_scale)))
    merge_y = others(merge_half, "y")
    columns = prepared(
        columns_kernel,
        (T, 2 * T + FF_DEV),
        (
            direct_weight,
            row(direct_scale),
            value_weight,
            row(value_scale),
            expand_weight,
            row(expand_scale),
        ),
    )
    columns_x = (columns, *others(columns, "x"))
    normed = prepared(
        norm_kernel,
        (D + PACK, T),
        (
            tokens,
            row(mixer_gain),
            spatial_weight.reshape(2 * T, T),
            row(value_gain),
            row(value_shift),
            spatial_bias,
        ),
    )
    near_rows, far_rows, back_rows = others(normed, "y")
    rows = prepared(
        rows_kernel, (4 * T + FF_DEV, T), (reduce_weight, row(reduce_scale)), (merge_half, *merge_y)
    )
    rows_z = (rows, *others(rows, ZRING))
    dv_stack, expand_stack = call(
        split_columns_kernel, [((4, T, 2 * T), BF), ((4, T, FF_DEV), BF)], columns_x, [VM] * 4, []
    )
    dv_own = joined((dv_stack, *others(dv_stack, ZRING)))
    dv_partner = swap(dv_own)
    merge_stack, reduce_stack = call(
        split_rows_kernel, [((4, 4 * T, T), BF), ((4, FF_DEV, T), BF)], rows_z, [VM] * 4, []
    )
    merge_own = joined((merge_stack, *others(merge_stack, "x")))
    merge_partner = swap(merge_own)
    expands = around(expand_stack, ZRING)
    reduces = around(reduce_stack, "x")

    parts, pack_own = call(
        dv_kernel,
        [((4, T, 4 * T), BF), ((4, PACK, T), BF)],
        (idx, dv_own, dv_partner, normed, near_rows, far_rows, back_rows),
        [SM] + [HB] * 6,
        [
            pltpu.VMEM((D, 4 * T), BF),
            pltpu.VMEM((4, T, D), BF),
            pltpu.SemaphoreType.DMA(()),
        ],
        [VM, HB],
        16,
    )
    parts = lax.all_to_all(parts, "y", 0, 0, tiled=True)
    pack_partner = swap(pack_own)

    middle, normed = call(
        mixer_kernel,
        [((T, D), BF), ((T, D), BF)],
        (
            idx,
            tokens,
            channel_gain.reshape(1, D),
            parts,
            pack_own,
            pack_partner,
            merge_own,
            merge_partner,
        ),
        [SM] + [VM] * 5 + [HB] * 2,
        [pltpu.VMEM((AW, D), BF), pltpu.VMEM((T, AW), BF), pltpu.SemaphoreType.DMA(())],
        None,
        16,
    )
    near_rows, far_rows, back_rows = others(normed, "y")
    dma = [pltpu.SemaphoreType.DMA(())]
    (up,) = call(up_kernel, [((D, 2 * FF_DEV), BF)], (idx, *expands), [SM] + [HB] * 4, dma)
    (down,) = call(down_kernel, [((2 * FF_DEV, D), BF)], (idx, *reduces), [SM] + [HB] * 4, dma)
    far_low, far_high = ff(up, down, (far_rows,), HALF)
    near, back = ff(up, down, (near_rows, back_rows))
    (own,) = ff(up, down, (normed,))
    relay_low = shift(far_low, "y", 1)
    relay_high = shift(far_high, "y", -1)
    near, back = call(
        plus_kernel, [((T, D), BF)] * 2, (near, back, relay_low, relay_high), [VM] * 4, []
    )
    got_back = shift(near, "y", 1)
    got_near = shift(back, "y", -1)
    lower = own.astype(F32) + (got_back.astype(F32) + got_near.astype(F32))
    return (middle.astype(F32) + lower).astype(BF)


def solution(mesh):
    finer = Mesh(mesh.devices.reshape(2, 4, 4, 4, 2), ALL)
    in_specs = (
        P(ALL, None),
        P(),
        P(FS, TP),
        P(TP),
        P(FS, TP),
        P(TP),
        P(TP),
        P(TP),
        P(TP, None, None),
        P(TP, None),
        P(TP, FS),
        P(FS),
        P(),
        P(FS, TP),
        P(TP),
        P(TP, FS),
        P(FS),
    )
    return jax.shard_map(layer, mesh=finer, in_specs=in_specs, out_specs=P(ALL, None), check_vma=False)
```

```python
import jax
import jax.numpy as jnp
from jax import lax
from jax.experimental import pallas as pl
from jax.experimental.pallas import tpu as pltpu
from jax.sharding import Mesh
from jax.sharding import PartitionSpec as P

ALL = ("rep", "z", "x", "y", "core")
FS = ("z", "x")
TP = ("y", "core")
ZRING = ("rep", "z")
EPS = 1e-06
BF = jnp.bfloat16
F32 = jnp.float32
T = 128
HALF = T // 2
D = 2048
AW = 1024
FF_DEV = 1024
K = D // T
PACK = 3 * T + 16
CHUNK = 512


def shift(x, axis, by):
    n = 8 if axis == ZRING else lax.axis_size(axis)
    pairs = [(i, (i + by) % n) for i in range(n)]
    if axis == ZRING and by == 2:
        pairs = [(i, (i + (2 if i % 2 == 0 else -2)) % n) for i in range(n)]
    return lax.ppermute(x, axis, pairs)


def swap(x):
    return lax.ppermute(x, "core", [(0, 1), (1, 0)])


def others(x, axis):
    return (shift(x, axis, -1), shift(x, axis, 2), shift(x, axis, 1))


def gelu(x):
    return 0.5 * x * (1.0 + jnp.tanh(0.7978845608028654 * (x + 0.044715 * x * x * x)))


VM = pl.BlockSpec(memory_space=pltpu.VMEM)
SM = pl.BlockSpec(memory_space=pltpu.SMEM)
HB = pl.BlockSpec(memory_space=pl.ANY)
RAW = pl.BlockSpec(memory_space=pltpu.HBM)


def call(kernel, outs, inputs, specs, scratch, out_specs=None, vmem=8, aliases={}):
    return pl.pallas_call(
        kernel,
        out_shape=[jax.ShapeDtypeStruct(s, d) for s, d in outs],
        in_specs=specs,
        out_specs=out_specs or [VM] * len(outs),
        scratch_shapes=scratch,
        input_output_aliases=aliases,
        compiler_params=pltpu.CompilerParams(vmem_limit_bytes=vmem * 1024 * 1024),
    )(*inputs)


def rms(floats, gain):
    return floats * lax.rsqrt(jnp.mean(floats * floats, axis=-1, keepdims=True) + EPS) * gain


def rows_of(first, second):
    high = first.astype(BF).astype(F32)
    other = second.astype(BF).astype(F32)
    return [high, first - high, other, second - other]


def copies(pairs, sem):
    started = [pltpu.make_async_copy(src, dst, sem) for src, dst in pairs]
    for c in started:
        c.start()
    return started


def finish(started):
    for c in started:
        c.wait()


def loaded(sources, buffers, sem):
    finish(copies(list(zip(sources, buffers)), sem))


def norm_kernel(*refs):
    sources, out, buffers, sem = refs[:6], refs[6], refs[7:13], refs[13]
    loaded(sources, buffers, sem)
    tokens, gain, spatial, value_gain, value_shift, bias = buffers
    normed = rms(tokens[...].astype(F32), gain[...]).astype(BF)
    for k in range(K):
        out[k * T : (k + 1) * T] = normed[:, k * T : (k + 1) * T]
    out[D : D + 2 * T] = spatial[...]
    tall = jnp.concatenate([*rows_of(bias[0:1], bias[1:2]), jnp.zeros((T - 4, T), F32)], axis=0)
    out[D + 2 * T : D + 3 * T] = tall.T.astype(BF)
    gains = [*rows_of(value_gain[...], value_shift[...]), jnp.zeros((12, T), F32)]
    out[D + 3 * T : D + PACK] = jnp.concatenate(gains, axis=0).astype(BF)


def columns_kernel(*refs):
    sources, out, buffers, sem = refs[:6], refs[6], refs[7:13], refs[13]
    loaded(sources, buffers, sem)
    at = 0
    for weight, scale in zip(buffers[0::2], buffers[1::2]):
        width = weight.shape[1]
        out[:, at : at + width] = (weight[...] * scale[...]).astype(BF)
        at += width


def rows_kernel(*refs):
    sources, out, buffers, sem = refs[:4], refs[4], refs[5:9], refs[9]
    loaded(sources, buffers, sem)
    out[:T] = (buffers[0][...] * buffers[1][...]).astype(BF)
    out[T:] = (buffers[2][...] * buffers[3][...]).astype(BF)


def split_columns_kernel(c0, c1, c2, c3, first, second):
    for n, part in enumerate((c0, c1, c2, c3)):
        first[n] = part[:, : first.shape[2]]
        second[n] = part[:, first.shape[2] :]


def split_rows_kernel(r0, r1, r2, r3, first, second):
    for n, part in enumerate((r0, r1, r2, r3)):
        first[n] = part[: first.shape[1]]
        second[n] = part[first.shape[1] :]


def plus_kernel(near, back, low, high, near_out, back_out):
    near_out[:HALF] = (near[:HALF].astype(F32) + low[...].astype(F32)).astype(BF)
    near_out[HALF:] = near[HALF:]
    back_out[:HALF] = back[:HALF]
    back_out[HALF:] = (back[HALF:].astype(F32) + high[...].astype(F32)).astype(BF)


def prepared(kernel, out, raw, ready=()):
    buffers = [pltpu.VMEM(a.shape, a.dtype) for a in raw]
    return call(
        kernel,
        [(out, BF)],
        (*ready, *[pltpu.with_memory_space_constraint(a, pltpu.HBM) for a in raw]),
        [VM] * len(ready) + [RAW] * len(raw),
        [*buffers, pltpu.SemaphoreType.DMA(())],
    )[0]


def place_of(idx, zr, xr):
    return lax.rem(idx[0] + zr, 4) * 4 + lax.rem(idx[1] + xr, 4)


def aligned(x):
    return pl.multiple_of(x * T, T)


def join_kernel(*refs):
    sources, out, sem = refs[:-2], refs[-2], refs[-1]
    pairs, at = [], 0
    for source in sources:
        pairs.append((source, out.at[at : at + source.shape[0]]))
        at += source.shape[0]
    finish(copies(pairs, sem))


def halves_kernel(near, back, low, high, sem):
    finish(copies([(back.at[:2], low), (near.at[2:], high)], sem))


def row_halves_kernel(near, back, low, high):
    low[...] = back[:HALF]
    high[...] = near[HALF:]


def joined(arrays):
    shape = (sum(a.shape[0] for a in arrays), *arrays[0].shape[1:])
    sem = [pltpu.SemaphoreType.DMA(())]
    return call(join_kernel, [(shape, BF)], arrays, [HB] * len(arrays), sem)[0]


def dv_kernel(idx, *refs):
    weights = refs[:2]
    sources = refs[2:6]
    out, pack, weight, rows, sem = refs[6:]
    pairs = []
    for q in range(2):
        for zr in range(4):
            for xr in range(4):
                row = aligned(place_of(idx, zr, xr))
                dst = weight.at[pl.ds(row, T), 2 * q * T : 2 * (q + 1) * T]
                pairs.append((weights[q].at[4 * zr + xr], dst))
    for g, source in enumerate(sources):
        pairs.append((source.at[D : D + PACK], pack.at[g]))
    started = copies(pairs, sem)

    def block(source, g, k):
        at = pl.multiple_of(k * T, T)
        return pltpu.make_async_copy(source.at[pl.ds(at, T)], rows.at[g, :, pl.ds(at, T)], sem)

    for g, source in enumerate(sources):
        pl.loop(0, K)(lambda k: block(source, g, k).start())
    finish(started)
    for g, source in enumerate(sources):
        pl.loop(0, K)(lambda k: block(source, g, k).wait())

    @pl.loop(0, 4)
    def _(g):
        part = jnp.dot(rows[g], weight[...], preferred_element_type=F32)
        out[lax.rem(idx[2] + g, 4)] = gelu(part).astype(BF)


def mixer_kernel(idx, *refs):
    merges, middle, normed, sem = refs[5:7], refs[7], refs[8], refs[9]
    tokens, gain, parts, pack_own, pack_partner, weight, gated, merge_sem = refs[10:]
    small = copies(list(zip(refs[:5], (tokens, gain, parts, pack_own, pack_partner))), sem)

    def placed(q, zr, xr, r):
        col = aligned(place_of(idx, zr, xr))
        dst = weight.at[pl.ds(aligned(4 * q + r), T), pl.ds(col, T)]
        return pltpu.make_async_copy(merges[q].at[16 * r + 4 * xr + zr], dst, merge_sem)

    places = [(q, zr, xr) for q in range(2) for zr in range(4) for xr in range(4)]

    @pl.loop(0, 4)
    def _(r):
        for place in places:
            placed(*place, r).start()

    finish(small)

    def moments(r, sums):
        value = [parts[r, :, (2 * q + 1) * T : (2 * q + 2) * T].astype(F32) for q in range(2)]
        total = jnp.sum(value[0] + value[1], axis=1, keepdims=True)
        squares = jnp.sum(value[0] * value[0] + value[1] * value[1], axis=1, keepdims=True)
        return sums[0] + total, sums[1] + squares

    nothing = jnp.zeros((T, 1), F32)
    total, squares = lax.fori_loop(0, 4, moments, (nothing, nothing))
    mean = total * (1.0 / AW)
    var = squares * (1.0 / AW) - mean * mean
    scale = lax.rsqrt(var + EPS)
    lane = lax.broadcasted_iota(jnp.int32, (T, T), 1)

    @pl.loop(0, 4)
    def _(r):
        y = lax.rem(idx[2] + r, 4)
        for q, pack in enumerate((pack_own, pack_partner)):
            gains = pack[r, 3 * T : 3 * T + 16].astype(F32)
            gain_row = gains[0:1] + gains[1:2]
            shift_row = gains[2:3] + gains[3:4]
            bias = pack[r, 2 * T : 3 * T].astype(F32)
            bias_low = bias[:, 0:1] + bias[:, 1:2]
            bias_high = bias[:, 2:3] + bias[:, 3:4]
            value = parts[y, :, (2 * q + 1) * T : (2 * q + 2) * T].astype(F32)
            ready = ((value - mean) * scale * gain_row + shift_row).astype(BF)
            left = jnp.dot(pack[r, 0:T], ready, preferred_element_type=F32) + bias_low
            right = jnp.dot(pack[r, T : 2 * T], ready, preferred_element_type=F32) + bias_high
            mixed = jnp.where(lane < T // 2, left, right)
            direct = parts[y, :, 2 * q * T : (2 * q + 1) * T].astype(F32)
            gated[:, pl.ds(pl.multiple_of((4 * q + r) * T, T), T)] = (direct * mixed).astype(BF)


    @pl.loop(0, 4)
    def _(r):
        for place in places:
            placed(*place, r).wait()

    @pl.loop(0, D // CHUNK)
    def _(n):
        cols = pl.ds(pl.multiple_of(n * CHUNK, CHUNK), CHUNK)
        mix = jnp.dot(gated[...], weight[:, cols], preferred_element_type=F32)
        middle[:, cols] = (tokens[:, cols].astype(F32) + mix).astype(BF)

    normed[...] = rms(middle[...].astype(F32), gain[...]).astype(BF)


def picked(parts, n, k):
    near, far = parts
    return far.at[k] if n == 2 else near.at[(0, 4, None, 8)[n] + k]


def up_kernel(idx, *refs):
    out, sem = refs[4:]
    pairs = []
    for q in range(2):
        for zr in range(4):
            for xr in range(4):
                at = aligned(place_of(idx, zr, xr))
                dst = out.at[pl.ds(at, T), q * FF_DEV : (q + 1) * FF_DEV]
                pairs.append((picked(refs[2 * q : 2 * q + 2], zr, xr), dst))
    finish(copies(pairs, sem))


def down_place(out, at, q):
    return out.at[q * FF_DEV : (q + 1) * FF_DEV, pl.ds(aligned(at), T)]


def down_first_kernel(idx, *refs):
    out, sem = refs[2:]
    pairs = []
    for q in range(2):
        for n, xr in enumerate((0, 1, 3)):
            for zr in range(4):
                pairs.append((refs[q].at[4 * n + zr], down_place(out, place_of(idx, zr, xr), q)))
    finish(copies(pairs, sem))


def down_last_kernel(idx, own, partner, _, out, sem):
    pairs = []
    for q, source in enumerate((own, partner)):
        for zr in range(4):
            pairs.append((source.at[zr], down_place(out, place_of(idx, zr, 2), q)))
    finish(copies(pairs, sem))


def ff_kernel(count, up, down, *refs):
    tokens, outs = refs[:count], refs[count:-2]
    rows, hidden = refs[-2:]
    at = 0
    for t in tokens:
        rows[at : at + t.shape[0]] = t[...]
        at += t.shape[0]

    @pl.loop(0, D // CHUNK)
    def _(n):
        cols = pl.ds(pl.multiple_of(n * CHUNK, CHUNK), CHUNK)
        pre = jnp.dot(rows[...], up[:, cols], preferred_element_type=F32)
        hidden[:, cols] = jnp.square(jnp.maximum(pre, 0.0)).astype(BF)

    @pl.loop(0, D // CHUNK)
    def _(n):
        cols = pl.ds(pl.multiple_of(n * CHUNK, CHUNK), CHUNK)
        part = jnp.dot(hidden[...], down[:, cols], preferred_element_type=F32).astype(BF)
        size = outs[0].shape[0]
        for g, out in enumerate(outs):
            out[:, cols] = part[g * size : (g + 1) * size]


def ff(up, down, tokens, size=T):
    height = sum(t.shape[0] for t in tokens)
    return call(
        lambda *refs: ff_kernel(len(tokens), *refs),
        [((size, D), BF)] * (height // size),
        (up, down, *tokens),
        [VM] * (2 + len(tokens)),
        [pltpu.VMEM((height, D), BF), pltpu.VMEM((height, D), BF)],
    )


def around(stack, second):
    near = shift(stack, second, -1)
    back = shift(stack, second, 1)
    low, high = call(
        halves_kernel,
        [((2, *stack.shape[1:]), BF)] * 2,
        (near, back),
        [HB] * 2,
        [pltpu.SemaphoreType.DMA(())],
    )
    far_low = shift(low, second, 1)
    far_high = shift(high, second, -1)
    mine = (joined((stack, near, back)), joined((far_low, far_high)))
    return (*mine, *[swap(m) for m in mine])


def layer(
    tokens,
    mixer_gain,
    direct_weight,
    direct_scale,
    value_weight,
    value_scale,
    value_gain,
    value_shift,
    spatial_weight,
    spatial_bias,
    merge_weight,
    merge_scale,
    channel_gain,
    expand_weight,
    expand_scale,
    reduce_weight,
    reduce_scale,
):
    idx = jnp.stack([lax.axis_index(a) for a in ("z", "x", "y")]).astype(jnp.int32)
    row = lambda v: v.reshape(1, -1)
    columns = prepared(
        columns_kernel,
        (T, 2 * T + FF_DEV),
        (
            direct_weight,
            row(direct_scale),
            value_weight,
            row(value_scale),
            expand_weight,
            row(expand_scale),
        ),
    )
    columns_x = (columns, *others(columns, "x"))
    normed = prepared(
        norm_kernel,
        (D + PACK, T),
        (
            tokens,
            row(mixer_gain),
            spatial_weight.reshape(2 * T, T),
            row(value_gain),
            row(value_shift),
            spatial_bias,
        ),
    )
    near_rows, far_rows, back_rows = others(normed, "y")
    rows = prepared(
        rows_kernel,
        (T + FF_DEV, T),
        (merge_weight, row(merge_scale), reduce_weight, row(reduce_scale)),
    )
    rows_z = (rows, *others(rows, ZRING))
    dv_stack, expand_stack = call(
        split_columns_kernel, [((4, T, 2 * T), BF), ((4, T, FF_DEV), BF)], columns_x, [VM] * 4, []
    )
    dv_own = joined((dv_stack, *others(dv_stack, ZRING)))
    dv_partner = swap(dv_own)
    merge_stack, reduce_stack = call(
        split_rows_kernel, [((4, T, T), BF), ((4, FF_DEV, T), BF)], rows_z, [VM] * 4, []
    )
    merge_mine = joined((merge_stack, *others(merge_stack, "x")))
    merge_own = joined((merge_mine, *others(merge_mine, "y")))
    merge_partner = swap(merge_own)
    expands = around(expand_stack, ZRING)
    reduces = around(reduce_stack, "x")

    parts, pack_own = call(
        dv_kernel,
        [((4, T, 4 * T), BF), ((4, PACK, T), BF)],
        (idx, dv_own, dv_partner, normed, near_rows, far_rows, back_rows),
        [SM] + [HB] * 6,
        [
            pltpu.VMEM((D, 4 * T), BF),
            pltpu.VMEM((4, T, D), BF),
            pltpu.SemaphoreType.DMA(()),
        ],
        [VM, HB],
        16,
    )
    parts = lax.all_to_all(parts, "y", 0, 0, tiled=True)
    pack_partner = swap(pack_own)

    middle, normed = call(
        mixer_kernel,
        [((T, D), BF), ((T, D), BF)],
        (
            idx,
            pltpu.with_memory_space_constraint(tokens, pltpu.HBM),
            pltpu.with_memory_space_constraint(row(channel_gain), pltpu.HBM),
            parts,
            pack_own,
            pack_partner,
            merge_own,
            merge_partner,
        ),
        [SM] + [HB] * 7,
        [
            pltpu.SemaphoreType.DMA(()),
            pltpu.VMEM((T, D), BF),
            pltpu.VMEM((1, D), F32),
            pltpu.VMEM((4, T, 4 * T), BF),
            pltpu.VMEM((4, PACK, T), BF),
            pltpu.VMEM((4, PACK, T), BF),
            pltpu.VMEM((AW, D), BF),
            pltpu.VMEM((T, AW), BF),
            pltpu.SemaphoreType.DMA(()),
        ],
        None,
        16,
    )
    near_rows, back_rows = shift(normed, "y", -1), shift(normed, "y", 1)
    low, high = call(row_halves_kernel, [((HALF, D), BF)] * 2, (near_rows, back_rows), [VM] * 2, [])
    far_rows = shift(low, "y", 1), shift(high, "y", -1)
    dma = [pltpu.SemaphoreType.DMA(())]
    (up,) = call(up_kernel, [((D, 2 * FF_DEV), BF)], (idx, *expands), [SM] + [HB] * 4, dma)
    whole = [((2 * FF_DEV, D), BF)]
    near_own, far_own, near_partner, far_partner = reduces
    (down,) = call(down_first_kernel, whole, (idx, near_own, near_partner), [SM, HB, HB], dma)
    (down,) = call(
        down_last_kernel,
        whole,
        (idx, far_own, far_partner, down),
        [SM, HB, HB, VM],
        dma,
        aliases={3: 0},
    )
    far_low, far_high = ff(up, down, far_rows, HALF)
    near, back = ff(up, down, (near_rows, back_rows))
    (own,) = ff(up, down, (normed,))
    relay_low = shift(far_low, "y", 1)
    relay_high = shift(far_high, "y", -1)
    near, back = call(
        plus_kernel, [((T, D), BF)] * 2, (near, back, relay_low, relay_high), [VM] * 4, []
    )
    got_back = shift(near, "y", 1)
    got_near = shift(back, "y", -1)
    lower = own.astype(F32) + (got_back.astype(F32) + got_near.astype(F32))
    return (middle.astype(F32) + lower).astype(BF)


def solution(mesh):
    finer = Mesh(mesh.devices.reshape(2, 4, 4, 4, 2), ALL)
    in_specs = (
        P(ALL, None),
        P(),
        P(FS, TP),
        P(TP),
        P(FS, TP),
        P(TP),
        P(TP),
        P(TP),
        P(TP, None, None),
        P(TP, None),
        P(TP, FS),
        P(FS),
        P(),
        P(FS, TP),
        P(TP),
        P(TP, FS),
        P(FS),
    )
    return jax.shard_map(layer, mesh=finer, in_specs=in_specs, out_specs=P(ALL, None), check_vma=False)
```

```python
import jax
import jax.numpy as jnp
from jax import lax
from jax.experimental import pallas as pl
from jax.experimental.pallas import tpu as pltpu
from jax.sharding import Mesh
from jax.sharding import PartitionSpec as P

ALL = ("rep", "z", "x", "y", "core")
FS = ("z", "x")
TP = ("y", "core")
ZRING = ("rep", "z")
EPS = 1e-06
BF = jnp.bfloat16
F32 = jnp.float32
T = 128
HALF = T // 2
D = 2048
AW = 1024
FF_DEV = 1024
K = D // T
PACK = 3 * T + 16
CHUNK = 512


def shift(x, axis, by):
    n = 8 if axis == ZRING else lax.axis_size(axis)
    pairs = [(i, (i + by) % n) for i in range(n)]
    if axis == ZRING and by == 2:
        pairs = [(i, (i + (2 if i % 2 == 0 else -2)) % n) for i in range(n)]
    return lax.ppermute(x, axis, pairs)


def swap(x):
    return lax.ppermute(x, "core", [(0, 1), (1, 0)])


def others(x, axis):
    return (shift(x, axis, -1), shift(x, axis, 2), shift(x, axis, 1))


def gelu(x):
    return 0.5 * x * (1.0 + jnp.tanh(0.7978845608028654 * (x + 0.044715 * x * x * x)))


VM = pl.BlockSpec(memory_space=pltpu.VMEM)
SM = pl.BlockSpec(memory_space=pltpu.SMEM)
HB = pl.BlockSpec(memory_space=pl.ANY)
RAW = pl.BlockSpec(memory_space=pltpu.HBM)


def call(kernel, outs, inputs, specs, scratch, out_specs=None, vmem=8, aliases={}):
    return pl.pallas_call(
        kernel,
        out_shape=[jax.ShapeDtypeStruct(s, d) for s, d in outs],
        in_specs=specs,
        out_specs=out_specs or [VM] * len(outs),
        scratch_shapes=scratch,
        input_output_aliases=aliases,
        compiler_params=pltpu.CompilerParams(vmem_limit_bytes=vmem * 1024 * 1024),
    )(*inputs)


def rms(floats, gain):
    return floats * lax.rsqrt(jnp.mean(floats * floats, axis=-1, keepdims=True) + EPS) * gain


def rows_of(first, second):
    high = first.astype(BF).astype(F32)
    other = second.astype(BF).astype(F32)
    return [high, first - high, other, second - other]


def copies(pairs, sem):
    started = [pltpu.make_async_copy(src, dst, sem) for src, dst in pairs]
    for c in started:
        c.start()
    return started


def finish(started):
    for c in started:
        c.wait()


def loaded(sources, buffers, sem):
    finish(copies(list(zip(sources, buffers)), sem))


def norm_kernel(*refs):
    sources, out, buffers, sem = refs[:6], refs[6], refs[7:13], refs[13]
    loaded(sources, buffers, sem)
    tokens, gain, spatial, value_gain, value_shift, bias = buffers
    normed = rms(tokens[...].astype(F32), gain[...]).astype(BF)
    for k in range(K):
        out[k * T : (k + 1) * T] = normed[:, k * T : (k + 1) * T]
    out[D : D + 2 * T] = spatial[...]
    tall = jnp.concatenate([*rows_of(bias[0:1], bias[1:2]), jnp.zeros((T - 4, T), F32)], axis=0)
    out[D + 2 * T : D + 3 * T] = tall.T.astype(BF)
    gains = [*rows_of(value_gain[...], value_shift[...]), jnp.zeros((12, T), F32)]
    out[D + 3 * T : D + PACK] = jnp.concatenate(gains, axis=0).astype(BF)


def columns_kernel(*refs):
    sources, out, buffers, sem = refs[:6], refs[6], refs[7:13], refs[13]
    loaded(sources, buffers, sem)
    at = 0
    for weight, scale in zip(buffers[0::2], buffers[1::2]):
        width = weight.shape[1]
        out[:, at : at + width] = (weight[...] * scale[...]).astype(BF)
        at += width


def rows_kernel(*refs):
    sources, out, buffers, sem = refs[:4], refs[4], refs[5:9], refs[9]
    loaded(sources, buffers, sem)
    out[:T] = (buffers[0][...] * buffers[1][...]).astype(BF)
    out[T:] = (buffers[2][...] * buffers[3][...]).astype(BF)


def split_columns_kernel(c0, c1, c2, c3, first, second):
    for n, part in enumerate((c0, c1, c2, c3)):
        first[n] = part[:, : first.shape[2]]
        second[n] = part[:, first.shape[2] :]


def split_rows_kernel(r0, r1, r2, r3, first, second):
    for n, part in enumerate((r0, r1, r2, r3)):
        first[n] = part[: first.shape[1]]
        second[n] = part[first.shape[1] :]


def plus_kernel(near, back, low, high, near_out, back_out):
    near_out[:HALF] = (near[:HALF].astype(F32) + low[...].astype(F32)).astype(BF)
    near_out[HALF:] = near[HALF:]
    back_out[:HALF] = back[:HALF]
    back_out[HALF:] = (back[HALF:].astype(F32) + high[...].astype(F32)).astype(BF)


def prepared(kernel, out, raw, ready=()):
    buffers = [pltpu.VMEM(a.shape, a.dtype) for a in raw]
    return call(
        kernel,
        [(out, BF)],
        (*ready, *[pltpu.with_memory_space_constraint(a, pltpu.HBM) for a in raw]),
        [VM] * len(ready) + [RAW] * len(raw),
        [*buffers, pltpu.SemaphoreType.DMA(())],
    )[0]


def place_of(idx, zr, xr):
    return lax.rem(idx[0] + zr, 4) * 4 + lax.rem(idx[1] + xr, 4)


def aligned(x):
    return pl.multiple_of(x * T, T)


def join_kernel(*refs):
    sources, out, sem = refs[:-2], refs[-2], refs[-1]
    pairs, at = [], 0
    for source in sources:
        pairs.append((source, out.at[at : at + source.shape[0]]))
        at += source.shape[0]
    finish(copies(pairs, sem))


def halves_kernel(near, back, low, high, sem):
    finish(copies([(back.at[:2], low), (near.at[2:], high)], sem))


def row_halves_kernel(near, back, low, high):
    low[...] = back[:HALF]
    high[...] = near[HALF:]


def joined(arrays):
    shape = (sum(a.shape[0] for a in arrays), *arrays[0].shape[1:])
    sem = [pltpu.SemaphoreType.DMA(())]
    return call(join_kernel, [(shape, BF)], arrays, [HB] * len(arrays), sem)[0]


def dv_kernel(idx, *refs):
    weights = refs[:2]
    sources = refs[2:6]
    out, pack, weight, rows, sem = refs[6:]
    pairs = []
    for q in range(2):
        for zr in range(4):
            for xr in range(4):
                row = aligned(place_of(idx, zr, xr))
                dst = weight.at[pl.ds(row, T), 2 * q * T : 2 * (q + 1) * T]
                pairs.append((weights[q].at[4 * zr + xr], dst))
    for g, source in enumerate(sources):
        pairs.append((source.at[D : D + PACK], pack.at[g]))
    started = copies(pairs, sem)

    def block(source, g, k):
        at = pl.multiple_of(k * T, T)
        return pltpu.make_async_copy(source.at[pl.ds(at, T)], rows.at[g, :, pl.ds(at, T)], sem)

    for g, source in enumerate(sources):
        pl.loop(0, K)(lambda k: block(source, g, k).start())
    finish(started)
    for g, source in enumerate(sources):
        pl.loop(0, K)(lambda k: block(source, g, k).wait())

    @pl.loop(0, 4)
    def _(g):
        part = jnp.dot(rows[g], weight[...], preferred_element_type=F32)
        out[lax.rem(idx[2] + g, 4)] = gelu(part).astype(BF)


def mixer_kernel(idx, *refs):
    merges, middle, normed, sem = refs[5:9], refs[9], refs[10], refs[11]
    tokens, gain, parts, pack_own, pack_partner, weight, gated, merge_sem = refs[12:]
    small = copies(list(zip(refs[:5], (tokens, gain, parts, pack_own, pack_partner))), sem)

    def placed(n, q, r):
        zr, xr = lax.div(n, 4), lax.rem(n, 4)
        source = merges[2 * q + min(r, 1)].at[16 * max(r - 1, 0) + 4 * xr + zr]
        at = (4 * q + r) * T
        dst = weight.at[at : at + T, pl.ds(aligned(place_of(idx, zr, xr)), T)]
        return pltpu.make_async_copy(source, dst, merge_sem)

    pieces = [(q, r) for q in range(2) for r in range(4)]

    @pl.loop(0, 16)
    def _(n):
        for piece in pieces:
            placed(n, *piece).start()

    finish(small)

    def moments(r, sums):
        value = [parts[r, :, (2 * q + 1) * T : (2 * q + 2) * T].astype(F32) for q in range(2)]
        total = jnp.sum(value[0] + value[1], axis=1, keepdims=True)
        squares = jnp.sum(value[0] * value[0] + value[1] * value[1], axis=1, keepdims=True)
        return sums[0] + total, sums[1] + squares

    nothing = jnp.zeros((T, 1), F32)
    total, squares = lax.fori_loop(0, 4, moments, (nothing, nothing))
    mean = total * (1.0 / AW)
    var = squares * (1.0 / AW) - mean * mean
    scale = lax.rsqrt(var + EPS)
    lane = lax.broadcasted_iota(jnp.int32, (T, T), 1)

    @pl.loop(0, 4)
    def _(r):
        y = lax.rem(idx[2] + r, 4)
        for q, pack in enumerate((pack_own, pack_partner)):
            gains = pack[r, 3 * T : 3 * T + 16].astype(F32)
            gain_row = gains[0:1] + gains[1:2]
            shift_row = gains[2:3] + gains[3:4]
            bias = pack[r, 2 * T : 3 * T].astype(F32)
            bias_low = bias[:, 0:1] + bias[:, 1:2]
            bias_high = bias[:, 2:3] + bias[:, 3:4]
            value = parts[y, :, (2 * q + 1) * T : (2 * q + 2) * T].astype(F32)
            ready = ((value - mean) * scale * gain_row + shift_row).astype(BF)
            left = jnp.dot(pack[r, 0:T], ready, preferred_element_type=F32) + bias_low
            right = jnp.dot(pack[r, T : 2 * T], ready, preferred_element_type=F32) + bias_high
            mixed = jnp.where(lane < T // 2, left, right)
            direct = parts[y, :, 2 * q * T : (2 * q + 1) * T].astype(F32)
            gated[:, pl.ds(pl.multiple_of((4 * q + r) * T, T), T)] = (direct * mixed).astype(BF)


    @pl.loop(0, 16)
    def _(n):
        for piece in pieces:
            placed(n, *piece).wait()

    @pl.loop(0, D // CHUNK)
    def _(n):
        cols = pl.ds(pl.multiple_of(n * CHUNK, CHUNK), CHUNK)
        mix = jnp.dot(gated[...], weight[:, cols], preferred_element_type=F32)
        middle[:, cols] = (tokens[:, cols].astype(F32) + mix).astype(BF)

    normed[...] = rms(middle[...].astype(F32), gain[...]).astype(BF)


def up_kernel(idx, *refs):
    out, sem = refs[4:]

    def placed(xr, q, zr):
        dst = out.at[pl.ds(aligned(place_of(idx, zr, xr)), T), q * FF_DEV : (q + 1) * FF_DEV]
        near, far = refs[2 * q : 2 * q + 2]
        source = far.at[xr] if zr == 2 else near.at[(0, 4, None, 8)[zr] + xr]
        return pltpu.make_async_copy(source, dst, sem)

    pieces = [(q, zr) for q in range(2) for zr in range(4)]

    @pl.loop(0, 4)
    def _(xr):
        for piece in pieces:
            placed(xr, *piece).start()

    @pl.loop(0, 4)
    def _(xr):
        for piece in pieces:
            placed(xr, *piece).wait()


def down_place(out, at, q):
    return out.at[q * FF_DEV : (q + 1) * FF_DEV, pl.ds(aligned(at), T)]


def down_first_kernel(idx, *refs):
    out, sem = refs[2:]

    def placed(zr, q, n):
        dst = down_place(out, place_of(idx, zr, (0, 1, 3)[n]), q)
        return pltpu.make_async_copy(refs[q].at[4 * n + zr], dst, sem)

    pieces = [(q, n) for q in range(2) for n in range(3)]

    @pl.loop(0, 4)
    def _(zr):
        for piece in pieces:
            placed(zr, *piece).start()

    @pl.loop(0, 4)
    def _(zr):
        for piece in pieces:
            placed(zr, *piece).wait()


def down_last_kernel(idx, own, partner, _, out, sem):
    pairs = []
    for q, source in enumerate((own, partner)):
        for zr in range(4):
            pairs.append((source.at[zr], down_place(out, place_of(idx, zr, 2), q)))
    finish(copies(pairs, sem))


def ff_kernel(count, up, down, *refs):
    tokens, outs = refs[:count], refs[count:-2]
    rows, hidden = refs[-2:]
    at = 0
    for t in tokens:
        rows[at : at + t.shape[0]] = t[...]
        at += t.shape[0]

    @pl.loop(0, D // CHUNK)
    def _(n):
        cols = pl.ds(pl.multiple_of(n * CHUNK, CHUNK), CHUNK)
        pre = jnp.dot(rows[...], up[:, cols], preferred_element_type=F32)
        hidden[:, cols] = jnp.square(jnp.maximum(pre, 0.0)).astype(BF)

    @pl.loop(0, D // CHUNK)
    def _(n):
        cols = pl.ds(pl.multiple_of(n * CHUNK, CHUNK), CHUNK)
        part = jnp.dot(hidden[...], down[:, cols], preferred_element_type=F32).astype(BF)
        size = outs[0].shape[0]
        for g, out in enumerate(outs):
            out[:, cols] = part[g * size : (g + 1) * size]


def ff(up, down, tokens, size=T):
    height = sum(t.shape[0] for t in tokens)
    return call(
        lambda *refs: ff_kernel(len(tokens), *refs),
        [((size, D), BF)] * (height // size),
        (up, down, *tokens),
        [VM] * (2 + len(tokens)),
        [pltpu.VMEM((height, D), BF), pltpu.VMEM((height, D), BF)],
    )


def around(stack, second):
    near = shift(stack, second, -1)
    back = shift(stack, second, 1)
    low, high = call(
        halves_kernel,
        [((2, *stack.shape[1:]), BF)] * 2,
        (near, back),
        [HB] * 2,
        [pltpu.SemaphoreType.DMA(())],
    )
    far_low = shift(low, second, 1)
    far_high = shift(high, second, -1)
    mine = (joined((stack, near, back)), joined((far_low, far_high)))
    return (*mine, *[swap(m) for m in mine])


def layer(
    tokens,
    mixer_gain,
    direct_weight,
    direct_scale,
    value_weight,
    value_scale,
    value_gain,
    value_shift,
    spatial_weight,
    spatial_bias,
    merge_weight,
    merge_scale,
    channel_gain,
    expand_weight,
    expand_scale,
    reduce_weight,
    reduce_scale,
):
    idx = jnp.stack([lax.axis_index(a) for a in ("z", "x", "y")]).astype(jnp.int32)
    row = lambda v: v.reshape(1, -1)
    columns = prepared(
        columns_kernel,
        (T, 2 * T + FF_DEV),
        (
            direct_weight,
            row(direct_scale),
            value_weight,
            row(value_scale),
            expand_weight,
            row(expand_scale),
        ),
    )
    columns_x = (columns, *others(columns, "x"))
    normed = prepared(
        norm_kernel,
        (D + PACK, T),
        (
            tokens,
            row(mixer_gain),
            spatial_weight.reshape(2 * T, T),
            row(value_gain),
            row(value_shift),
            spatial_bias,
        ),
    )
    near_rows, far_rows, back_rows = others(normed, "y")
    rows = prepared(
        rows_kernel,
        (T + FF_DEV, T),
        (merge_weight, row(merge_scale), reduce_weight, row(reduce_scale)),
    )
    rows_z = (rows, *others(rows, ZRING))
    dv_stack, expand_stack = call(
        split_columns_kernel, [((4, T, 2 * T), BF), ((4, T, FF_DEV), BF)], columns_x, [VM] * 4, []
    )
    dv_own = joined((dv_stack, *others(dv_stack, ZRING)))
    dv_partner = swap(dv_own)
    merge_stack, reduce_stack = call(
        split_rows_kernel, [((4, T, T), BF), ((4, FF_DEV, T), BF)], rows_z, [VM] * 4, []
    )
    merge_mine = joined((merge_stack, *others(merge_stack, "x")))
    merge_rest = joined(others(merge_mine, "y"))
    merges = (merge_mine, merge_rest, swap(merge_mine), swap(merge_rest))
    expands = around(expand_stack, ZRING)
    reduces = around(reduce_stack, "x")

    parts, pack_own = call(
        dv_kernel,
        [((4, T, 4 * T), BF), ((4, PACK, T), BF)],
        (idx, dv_own, dv_partner, normed, near_rows, far_rows, back_rows),
        [SM] + [HB] * 6,
        [
            pltpu.VMEM((D, 4 * T), BF),
            pltpu.VMEM((4, T, D), BF),
            pltpu.SemaphoreType.DMA(()),
        ],
        [VM, HB],
        16,
    )
    parts = lax.all_to_all(parts, "y", 0, 0, tiled=True)
    pack_partner = swap(pack_own)

    middle, normed = call(
        mixer_kernel,
        [((T, D), BF), ((T, D), BF)],
        (
            idx,
            pltpu.with_memory_space_constraint(tokens, pltpu.HBM),
            pltpu.with_memory_space_constraint(row(channel_gain), pltpu.HBM),
            parts,
            pack_own,
            pack_partner,
            *merges,
        ),
        [SM] + [HB] * 9,
        [
            pltpu.SemaphoreType.DMA(()),
            pltpu.VMEM((T, D), BF),
            pltpu.VMEM((1, D), F32),
            pltpu.VMEM((4, T, 4 * T), BF),
            pltpu.VMEM((4, PACK, T), BF),
            pltpu.VMEM((4, PACK, T), BF),
            pltpu.VMEM((AW, D), BF),
            pltpu.VMEM((T, AW), BF),
            pltpu.SemaphoreType.DMA(()),
        ],
        None,
        16,
    )
    near_rows, back_rows = shift(normed, "y", -1), shift(normed, "y", 1)
    low, high = call(row_halves_kernel, [((HALF, D), BF)] * 2, (near_rows, back_rows), [VM] * 2, [])
    far_rows = shift(low, "y", 1), shift(high, "y", -1)
    dma = [pltpu.SemaphoreType.DMA(())]
    (up,) = call(up_kernel, [((D, 2 * FF_DEV), BF)], (idx, *expands), [SM] + [HB] * 4, dma)
    whole = [((2 * FF_DEV, D), BF)]
    near_own, far_own, near_partner, far_partner = reduces
    (down,) = call(down_first_kernel, whole, (idx, near_own, near_partner), [SM, HB, HB], dma)
    (down,) = call(
        down_last_kernel,
        whole,
        (idx, far_own, far_partner, down),
        [SM, HB, HB, VM],
        dma,
        aliases={3: 0},
    )
    far_low, far_high = ff(up, down, far_rows, HALF)
    near, back = ff(up, down, (near_rows, back_rows))
    (own,) = ff(up, down, (normed,))
    relay_low = shift(far_low, "y", 1)
    relay_high = shift(far_high, "y", -1)
    near, back = call(
        plus_kernel, [((T, D), BF)] * 2, (near, back, relay_low, relay_high), [VM] * 4, []
    )
    got_back = shift(near, "y", 1)
    got_near = shift(back, "y", -1)
    lower = own.astype(F32) + (got_back.astype(F32) + got_near.astype(F32))
    return (middle.astype(F32) + lower).astype(BF)


def solution(mesh):
    finer = Mesh(mesh.devices.reshape(2, 4, 4, 4, 2), ALL)
    in_specs = (
        P(ALL, None),
        P(),
        P(FS, TP),
        P(TP),
        P(FS, TP),
        P(TP),
        P(TP),
        P(TP),
        P(TP, None, None),
        P(TP, None),
        P(TP, FS),
        P(FS),
        P(),
        P(FS, TP),
        P(TP),
        P(TP, FS),
        P(FS),
    )
    return jax.shard_map(layer, mesh=finer, in_specs=in_specs, out_specs=P(ALL, None), check_vma=False)
```

```python
import jax
import jax.numpy as jnp
from jax import lax
from jax.experimental import pallas as pl
from jax.experimental.pallas import tpu as pltpu
from jax.sharding import Mesh
from jax.sharding import PartitionSpec as P

ALL = ("rep", "z", "x", "y", "core")
FS = ("z", "x")
TP = ("y", "core")
ZRING = ("rep", "z")
EPS = 1e-06
BF = jnp.bfloat16
F32 = jnp.float32
T = 128
HALF = T // 2
D = 2048
AW = 1024
FF_DEV = 1024
K = D // T
PACK = 3 * T + 16
CHUNK = 512


def shift(x, axis, by):
    n = 8 if axis == ZRING else lax.axis_size(axis)
    pairs = [(i, (i + by) % n) for i in range(n)]
    if axis == ZRING and by == 2:
        pairs = [(i, (i + (2 if i % 2 == 0 else -2)) % n) for i in range(n)]
    return lax.ppermute(x, axis, pairs)


def swap(x):
    return lax.ppermute(x, "core", [(0, 1), (1, 0)])


def others(x, axis):
    return (shift(x, axis, -1), shift(x, axis, 2), shift(x, axis, 1))


def gelu(x):
    return 0.5 * x * (1.0 + jnp.tanh(0.7978845608028654 * (x + 0.044715 * x * x * x)))


VM = pl.BlockSpec(memory_space=pltpu.VMEM)
SM = pl.BlockSpec(memory_space=pltpu.SMEM)
HB = pl.BlockSpec(memory_space=pl.ANY)
RAW = pl.BlockSpec(memory_space=pltpu.HBM)


def call(kernel, outs, inputs, specs, scratch, out_specs=None, vmem=8, aliases={}):
    return pl.pallas_call(
        kernel,
        out_shape=[jax.ShapeDtypeStruct(s, d) for s, d in outs],
        in_specs=specs,
        out_specs=out_specs or [VM] * len(outs),
        scratch_shapes=scratch,
        input_output_aliases=aliases,
        compiler_params=pltpu.CompilerParams(vmem_limit_bytes=vmem * 1024 * 1024),
    )(*inputs)


def rms(floats, gain):
    return floats * lax.rsqrt(jnp.mean(floats * floats, axis=-1, keepdims=True) + EPS) * gain


def rows_of(first, second):
    high = first.astype(BF).astype(F32)
    other = second.astype(BF).astype(F32)
    return [high, first - high, other, second - other]


def copies(pairs, sem):
    started = [pltpu.make_async_copy(src, dst, sem) for src, dst in pairs]
    for c in started:
        c.start()
    return started


def finish(started):
    for c in started:
        c.wait()


def loaded(sources, buffers, sem):
    finish(copies(list(zip(sources, buffers)), sem))


def norm_kernel(*refs):
    sources, out, buffers, sem = refs[:6], refs[6], refs[7:13], refs[13]
    loaded(sources, buffers, sem)
    tokens, gain, spatial, value_gain, value_shift, bias = buffers
    normed = rms(tokens[...].astype(F32), gain[...]).astype(BF)
    for k in range(K):
        out[k * T : (k + 1) * T] = normed[:, k * T : (k + 1) * T]
    out[D : D + 2 * T] = spatial[...]
    tall = jnp.concatenate([*rows_of(bias[0:1], bias[1:2]), jnp.zeros((T - 4, T), F32)], axis=0)
    out[D + 2 * T : D + 3 * T] = tall.T.astype(BF)
    gains = [*rows_of(value_gain[...], value_shift[...]), jnp.zeros((12, T), F32)]
    out[D + 3 * T : D + PACK] = jnp.concatenate(gains, axis=0).astype(BF)


def columns_kernel(*refs):
    sources, out, buffers, sem = refs[:6], refs[6], refs[7:13], refs[13]
    loaded(sources, buffers, sem)
    at = 0
    for weight, scale in zip(buffers[0::2], buffers[1::2]):
        width = weight.shape[1]
        out[:, at : at + width] = (weight[...] * scale[...]).astype(BF)
        at += width


def rows_kernel(*refs):
    sources, out, buffers, sem = refs[:4], refs[4], refs[5:9], refs[9]
    loaded(sources, buffers, sem)
    out[:T] = (buffers[0][...] * buffers[1][...]).astype(BF)
    out[T:] = (buffers[2][...] * buffers[3][...]).astype(BF)


def split_columns_kernel(c0, c1, c2, c3, first, second):
    for n, part in enumerate((c0, c1, c2, c3)):
        first[n] = part[:, : first.shape[2]]
        second[n] = part[:, first.shape[2] :]


def split_rows_kernel(r0, r1, r2, r3, first, second):
    for n, part in enumerate((r0, r1, r2, r3)):
        first[n] = part[: first.shape[1]]
        second[n] = part[first.shape[1] :]


def plus_kernel(near, back, low, high, near_out, back_out):
    near_out[:HALF] = (near[:HALF].astype(F32) + low[...].astype(F32)).astype(BF)
    near_out[HALF:] = near[HALF:]
    back_out[:HALF] = back[:HALF]
    back_out[HALF:] = (back[HALF:].astype(F32) + high[...].astype(F32)).astype(BF)


def prepared(kernel, out, raw, ready=()):
    buffers = [pltpu.VMEM(a.shape, a.dtype) for a in raw]
    return call(
        kernel,
        [(out, BF)],
        (*ready, *[pltpu.with_memory_space_constraint(a, pltpu.HBM) for a in raw]),
        [VM] * len(ready) + [RAW] * len(raw),
        [*buffers, pltpu.SemaphoreType.DMA(())],
    )[0]


def place_of(idx, zr, xr):
    return lax.rem(idx[0] + zr, 4) * 4 + lax.rem(idx[1] + xr, 4)


def aligned(x):
    return pl.multiple_of(x * T, T)


def join_kernel(*refs):
    sources, out, sem = refs[:-2], refs[-2], refs[-1]
    pairs, at = [], 0
    for source in sources:
        pairs.append((source, out.at[at : at + source.shape[0]]))
        at += source.shape[0]
    finish(copies(pairs, sem))


def halves_kernel(near, back, low, high, sem):
    finish(copies([(back.at[:2], low), (near.at[2:], high)], sem))


def low_kernel(rows, out):
    out[...] = rows[:HALF]


def high_kernel(rows, out):
    out[...] = rows[HALF:]


def joined(arrays):
    shape = (sum(a.shape[0] for a in arrays), *arrays[0].shape[1:])
    sem = [pltpu.SemaphoreType.DMA(())]
    return call(join_kernel, [(shape, BF)], arrays, [HB] * len(arrays), sem)[0]


def dv_kernel(idx, *refs):
    weights = refs[:2]
    sources = refs[2:6]
    out, pack, weight, rows, sem = refs[6:]
    pairs = []
    for q in range(2):
        for zr in range(4):
            for xr in range(4):
                row = aligned(place_of(idx, zr, xr))
                dst = weight.at[pl.ds(row, T), 2 * q * T : 2 * (q + 1) * T]
                pairs.append((weights[q].at[4 * zr + xr], dst))
    for g, source in enumerate(sources):
        pairs.append((source.at[D : D + PACK], pack.at[g]))
    started = copies(pairs, sem)

    def block(source, g, k):
        at = pl.multiple_of(k * T, T)
        return pltpu.make_async_copy(source.at[pl.ds(at, T)], rows.at[g, :, pl.ds(at, T)], sem)

    for g, source in enumerate(sources):
        pl.loop(0, K)(lambda k: block(source, g, k).start())
    finish(started)
    for g, source in enumerate(sources):
        pl.loop(0, K)(lambda k: block(source, g, k).wait())

    @pl.loop(0, 4)
    def _(g):
        part = jnp.dot(rows[g], weight[...], preferred_element_type=F32)
        out[lax.rem(idx[2] + g, 4)] = gelu(part).astype(BF)


def mixer_kernel(idx, *refs):
    merges, middle, normed, sem = refs[5:9], refs[9], refs[10], refs[11]
    tokens, gain, parts, pack_own, pack_partner, weight, gated, merge_sem = refs[12:]
    small = copies(list(zip(refs[:5], (tokens, gain, parts, pack_own, pack_partner))), sem)

    def placed(n, q, r):
        zr, xr = lax.div(n, 4), lax.rem(n, 4)
        source = merges[2 * q + min(r, 1)].at[16 * max(r - 1, 0) + 4 * xr + zr]
        at = (4 * q + r) * T
        dst = weight.at[at : at + T, pl.ds(aligned(place_of(idx, zr, xr)), T)]
        return pltpu.make_async_copy(source, dst, merge_sem)

    pieces = [(q, r) for q in range(2) for r in range(4)]

    @pl.loop(0, 16)
    def _(n):
        for piece in pieces:
            placed(n, *piece).start()

    finish(small)

    def moments(r, sums):
        value = [parts[r, :, (2 * q + 1) * T : (2 * q + 2) * T].astype(F32) for q in range(2)]
        total = jnp.sum(value[0] + value[1], axis=1, keepdims=True)
        squares = jnp.sum(value[0] * value[0] + value[1] * value[1], axis=1, keepdims=True)
        return sums[0] + total, sums[1] + squares

    nothing = jnp.zeros((T, 1), F32)
    total, squares = lax.fori_loop(0, 4, moments, (nothing, nothing))
    mean = total * (1.0 / AW)
    var = squares * (1.0 / AW) - mean * mean
    scale = lax.rsqrt(var + EPS)
    lane = lax.broadcasted_iota(jnp.int32, (T, T), 1)

    @pl.loop(0, 4)
    def _(r):
        y = lax.rem(idx[2] + r, 4)
        for q, pack in enumerate((pack_own, pack_partner)):
            gains = pack[r, 3 * T : 3 * T + 16].astype(F32)
            gain_row = gains[0:1] + gains[1:2]
            shift_row = gains[2:3] + gains[3:4]
            bias = pack[r, 2 * T : 3 * T].astype(F32)
            bias_low = bias[:, 0:1] + bias[:, 1:2]
            bias_high = bias[:, 2:3] + bias[:, 3:4]
            value = parts[y, :, (2 * q + 1) * T : (2 * q + 2) * T].astype(F32)
            ready = ((value - mean) * scale * gain_row + shift_row).astype(BF)
            left = jnp.dot(pack[r, 0:T], ready, preferred_element_type=F32) + bias_low
            right = jnp.dot(pack[r, T : 2 * T], ready, preferred_element_type=F32) + bias_high
            mixed = jnp.where(lane < T // 2, left, right)
            direct = parts[y, :, 2 * q * T : (2 * q + 1) * T].astype(F32)
            gated[:, pl.ds(pl.multiple_of((4 * q + r) * T, T), T)] = (direct * mixed).astype(BF)


    @pl.loop(0, 16)
    def _(n):
        for piece in pieces:
            placed(n, *piece).wait()

    @pl.loop(0, D // CHUNK)
    def _(n):
        cols = pl.ds(pl.multiple_of(n * CHUNK, CHUNK), CHUNK)
        mix = jnp.dot(gated[...], weight[:, cols], preferred_element_type=F32)
        middle[:, cols] = (tokens[:, cols].astype(F32) + mix).astype(BF)

    normed[...] = rms(middle[...].astype(F32), gain[...]).astype(BF)


def up_kernel(idx, *refs):
    out, sem = refs[4:]

    def placed(xr, q, zr):
        dst = out.at[pl.ds(aligned(place_of(idx, zr, xr)), T), q * FF_DEV : (q + 1) * FF_DEV]
        near, far = refs[2 * q : 2 * q + 2]
        source = far.at[xr] if zr == 2 else near.at[(0, 4, None, 8)[zr] + xr]
        return pltpu.make_async_copy(source, dst, sem)

    pieces = [(q, zr) for q in range(2) for zr in range(4)]

    @pl.loop(0, 4)
    def _(xr):
        for piece in pieces:
            placed(xr, *piece).start()

    @pl.loop(0, 4)
    def _(xr):
        for piece in pieces:
            placed(xr, *piece).wait()


def down_place(out, at, q):
    return out.at[q * FF_DEV : (q + 1) * FF_DEV, pl.ds(aligned(at), T)]


def down_first_kernel(idx, *refs):
    out, sem = refs[2:]

    def placed(zr, q, n):
        dst = down_place(out, place_of(idx, zr, (0, 1, 3)[n]), q)
        return pltpu.make_async_copy(refs[q].at[4 * n + zr], dst, sem)

    pieces = [(q, n) for q in range(2) for n in range(3)]

    @pl.loop(0, 4)
    def _(zr):
        for piece in pieces:
            placed(zr, *piece).start()

    @pl.loop(0, 4)
    def _(zr):
        for piece in pieces:
            placed(zr, *piece).wait()


def down_last_kernel(idx, own, partner, _, out, sem):
    pairs = []
    for q, source in enumerate((own, partner)):
        for zr in range(4):
            pairs.append((source.at[zr], down_place(out, place_of(idx, zr, 2), q)))
    finish(copies(pairs, sem))


def ff_kernel(count, up, down, *refs):
    tokens, outs = refs[:count], refs[count:-2]
    rows, hidden = refs[-2:]
    at = 0
    for t in tokens:
        rows[at : at + t.shape[0]] = t[...]
        at += t.shape[0]

    @pl.loop(0, D // CHUNK)
    def _(n):
        cols = pl.ds(pl.multiple_of(n * CHUNK, CHUNK), CHUNK)
        pre = jnp.dot(rows[...], up[:, cols], preferred_element_type=F32)
        hidden[:, cols] = jnp.square(jnp.maximum(pre, 0.0)).astype(BF)

    @pl.loop(0, D // CHUNK)
    def _(n):
        cols = pl.ds(pl.multiple_of(n * CHUNK, CHUNK), CHUNK)
        part = jnp.dot(hidden[...], down[:, cols], preferred_element_type=F32).astype(BF)
        size = outs[0].shape[0]
        for g, out in enumerate(outs):
            out[:, cols] = part[g * size : (g + 1) * size]


def ff(up, down, tokens, size=T):
    height = sum(t.shape[0] for t in tokens)
    return call(
        lambda *refs: ff_kernel(len(tokens), *refs),
        [((size, D), BF)] * (height // size),
        (up, down, *tokens),
        [VM] * (2 + len(tokens)),
        [pltpu.VMEM((height, D), BF), pltpu.VMEM((height, D), BF)],
    )


def around(stack, second):
    near = shift(stack, second, -1)
    back = shift(stack, second, 1)
    low, high = call(
        halves_kernel,
        [((2, *stack.shape[1:]), BF)] * 2,
        (near, back),
        [HB] * 2,
        [pltpu.SemaphoreType.DMA(())],
    )
    far_low = shift(low, second, 1)
    far_high = shift(high, second, -1)
    mine = (joined((stack, near, back)), joined((far_low, far_high)))
    return (*mine, *[swap(m) for m in mine])


def layer(
    tokens,
    mixer_gain,
    direct_weight,
    direct_scale,
    value_weight,
    value_scale,
    value_gain,
    value_shift,
    spatial_weight,
    spatial_bias,
    merge_weight,
    merge_scale,
    channel_gain,
    expand_weight,
    expand_scale,
    reduce_weight,
    reduce_scale,
):
    idx = jnp.stack([lax.axis_index(a) for a in ("z", "x", "y")]).astype(jnp.int32)
    row = lambda v: v.reshape(1, -1)
    columns = prepared(
        columns_kernel,
        (T, 2 * T + FF_DEV),
        (
            direct_weight,
            row(direct_scale),
            value_weight,
            row(value_scale),
            expand_weight,
            row(expand_scale),
        ),
    )
    columns_x = (columns, *others(columns, "x"))
    normed = prepared(
        norm_kernel,
        (D + PACK, T),
        (
            tokens,
            row(mixer_gain),
            spatial_weight.reshape(2 * T, T),
            row(value_gain),
            row(value_shift),
            spatial_bias,
        ),
    )
    near_rows, far_rows, back_rows = others(normed, "y")
    rows = prepared(
        rows_kernel,
        (T + FF_DEV, T),
        (merge_weight, row(merge_scale), reduce_weight, row(reduce_scale)),
    )
    rows_z = (rows, *others(rows, ZRING))
    dv_stack, expand_stack = call(
        split_columns_kernel, [((4, T, 2 * T), BF), ((4, T, FF_DEV), BF)], columns_x, [VM] * 4, []
    )
    dv_own = joined((dv_stack, *others(dv_stack, ZRING)))
    dv_partner = swap(dv_own)
    merge_stack, reduce_stack = call(
        split_rows_kernel, [((4, T, T), BF), ((4, FF_DEV, T), BF)], rows_z, [VM] * 4, []
    )
    merge_mine = joined((merge_stack, *others(merge_stack, "x")))
    merge_rest = joined(others(merge_mine, "y"))
    merges = (merge_mine, merge_rest, swap(merge_mine), swap(merge_rest))
    expands = around(expand_stack, ZRING)
    reduces = around(reduce_stack, "x")

    parts, pack_own = call(
        dv_kernel,
        [((4, T, 4 * T), BF), ((4, PACK, T), BF)],
        (idx, dv_own, dv_partner, normed, near_rows, far_rows, back_rows),
        [SM] + [HB] * 6,
        [
            pltpu.VMEM((D, 4 * T), BF),
            pltpu.VMEM((4, T, D), BF),
            pltpu.SemaphoreType.DMA(()),
        ],
        [VM, HB],
        16,
    )
    parts = lax.all_to_all(parts, "y", 0, 0, tiled=True)
    pack_partner = swap(pack_own)

    middle, normed = call(
        mixer_kernel,
        [((T, D), BF), ((T, D), BF)],
        (
            idx,
            pltpu.with_memory_space_constraint(tokens, pltpu.HBM),
            pltpu.with_memory_space_constraint(row(channel_gain), pltpu.HBM),
            parts,
            pack_own,
            pack_partner,
            *merges,
        ),
        [SM] + [HB] * 9,
        [
            pltpu.SemaphoreType.DMA(()),
            pltpu.VMEM((T, D), BF),
            pltpu.VMEM((1, D), F32),
            pltpu.VMEM((4, T, 4 * T), BF),
            pltpu.VMEM((4, PACK, T), BF),
            pltpu.VMEM((4, PACK, T), BF),
            pltpu.VMEM((AW, D), BF),
            pltpu.VMEM((T, AW), BF),
            pltpu.SemaphoreType.DMA(()),
        ],
        None,
        16,
    )
    near_rows, back_rows = shift(normed, "y", -1), shift(normed, "y", 1)
    (high,) = call(high_kernel, [((HALF, D), BF)], (near_rows,), [VM], [])
    (low,) = call(low_kernel, [((HALF, D), BF)], (back_rows,), [VM], [])
    far_rows = shift(low, "y", 1), shift(high, "y", -1)
    dma = [pltpu.SemaphoreType.DMA(())]
    (up,) = call(up_kernel, [((D, 2 * FF_DEV), BF)], (idx, *expands), [SM] + [HB] * 4, dma)
    whole = [((2 * FF_DEV, D), BF)]
    near_own, far_own, near_partner, far_partner = reduces
    (down,) = call(down_first_kernel, whole, (idx, near_own, near_partner), [SM, HB, HB], dma)
    (down,) = call(
        down_last_kernel,
        whole,
        (idx, far_own, far_partner, down),
        [SM, HB, HB, VM],
        dma,
        aliases={3: 0},
    )
    far_low, far_high = ff(up, down, far_rows, HALF)
    near, back = ff(up, down, (near_rows, back_rows))
    (own,) = ff(up, down, (normed,))
    relay_low = shift(far_low, "y", 1)
    relay_high = shift(far_high, "y", -1)
    near, back = call(
        plus_kernel, [((T, D), BF)] * 2, (near, back, relay_low, relay_high), [VM] * 4, []
    )
    got_back = shift(near, "y", 1)
    got_near = shift(back, "y", -1)
    lower = own.astype(F32) + (got_back.astype(F32) + got_near.astype(F32))
    return (middle.astype(F32) + lower).astype(BF)


def solution(mesh):
    finer = Mesh(mesh.devices.reshape(2, 4, 4, 4, 2), ALL)
    in_specs = (
        P(ALL, None),
        P(),
        P(FS, TP),
        P(TP),
        P(FS, TP),
        P(TP),
        P(TP),
        P(TP),
        P(TP, None, None),
        P(TP, None),
        P(TP, FS),
        P(FS),
        P(),
        P(FS, TP),
        P(TP),
        P(TP, FS),
        P(FS),
    )
    return jax.shard_map(layer, mesh=finer, in_specs=in_specs, out_specs=P(ALL, None), check_vma=False)
```
